256 devices in a mesh: gr: 2 (over z_hi), fs: 16 (over z_lo, x), tp: 8 (over y, core).
Axes of the slice: x: 4, y: 4, z: 8 (z_hi: 2, z_lo: 4; z = z_hi * 4 + z_lo), core: 2. Of those that a mesh axis runs over, the one named last changes fastest.
Arguments:
- prompt: bfloat16 [16384, 2048], P(('gr', 'fs')), may hold values from -6 to 6
- gain_first: float32 [2048], P(('gr', 'fs')), may hold values from 0.1 to 1.9
- gate_first: float32 [2048, 2816], P(('gr', 'fs'), 'tp'), may hold values from -0.125 to 0.125
- up_first: float32 [2048, 2816], P(('gr', 'fs'), 'tp'), may hold values from -0.125 to 0.125
- down_first: float32 [2816, 2048], P(('gr', 'fs'), 'tp'), may hold values from -0.109375 to 0.109375
- gain_second: float32 [2048], P(('gr', 'fs')), may hold values from 0.1 to 1.9
- gate_second: float32 [2048, 2816], P(('gr', 'fs'), 'tp'), may hold values from -0.125 to 0.125
- up_second: float32 [2048, 2816], P(('gr', 'fs'), 'tp'), may hold values from -0.125 to 0.125
- down_second: float32 [2816, 2048], P(('gr', 'fs'), 'tp'), may hold values from -0.109375 to 0.109375
Outputs:
- serve_gate_first: bfloat16 [2048, 2816], P(None, 'tp')
- serve_up_first: bfloat16 [2048, 2816], P(None, 'tp')
- serve_down_first: bfloat16 [2816, 2048], P('tp')
- serve_gate_second: bfloat16 [2048, 2816], P(None, 'tp')
- serve_up_second: bfloat16 [2048, 2816], P(None, 'tp')
- serve_down_second: bfloat16 [2816, 2048], P('tp')
- mixed: bfloat16 [16384, 2048], P(('gr', 'fs', 'tp'))
The draws below stay inside these ranges and needn't reach their ends.
All inputs are finite; a program needn't handle non-finite values.
Results may differ from the reference program's by a relative error of at most 0.0085.
Values may be sent and summed in bfloat16 or wider, within the bound.
A program may use at most 128 MiB of HBM per device.

```python
import jax
import jax.numpy as jnp
from jax import lax

D = 2048
FF = 2816
TOKENS = 16384
N_TP = 8


def shard_levels(stream_key, dims, pieces, low, high):
    def one(dim, shards_of):
        steps = jax.random.uniform(jax.random.fold_in(jax.random.fold_in(stream_key, 6), dim), (shards_of,), jnp.float32, low / len(pieces), high / len(pieces))
        return jnp.repeat(jnp.exp(steps), dims[dim] // shards_of).reshape((-1,) + (1,) * (len(dims) - dim - 1))

    level = one(*pieces[0])
    for cut in pieces[1:]:
        level = level * one(*cut)
    return level


def normal_values(stream_key, shape, scale, most, pieces=(), dtype=jnp.bfloat16):
    gain = shard_levels(stream_key, shape, pieces, -0.22, 0.18) if pieces else 1.0
    result = jax.random.normal(stream_key, shape, jnp.float32) * scale * gain
    return jnp.minimum(jnp.maximum(result, -most), most).astype(dtype)


def setup_inputs(seed: int = 0) -> dict:
    keys = jax.random.split(jax.random.key(seed), 10)
    prompt = normal_values(keys[0], (TOKENS, D), 1.0, 6.0, ((0, 32),))
    gain_first = jnp.clip(1.0 + 0.18 * jax.random.normal(keys[1], (D,), jnp.float32), 0.1, 1.9)
    gate_first = normal_values(keys[2], (D, FF), D ** -0.5, 0.125, ((0, 32), (1, 8)), jnp.float32)
    up_first = normal_values(keys[3], (D, FF), D ** -0.5, 0.125, ((0, 32), (1, 8)), jnp.float32)
    down_first = normal_values(keys[4], (FF, D), FF ** -0.5, 0.109375, ((0, 32), (1, 8)), jnp.float32)
    gain_second = jnp.clip(1.0 + 0.18 * jax.random.normal(keys[5], (D,), jnp.float32), 0.1, 1.9)
    gate_second = normal_values(keys[6], (D, FF), D ** -0.5, 0.125, ((0, 32), (1, 8)), jnp.float32)
    up_second = normal_values(keys[7], (D, FF), D ** -0.5, 0.125, ((0, 32), (1, 8)), jnp.float32)
    down_second = normal_values(keys[8], (FF, D), FF ** -0.5, 0.109375, ((0, 32), (1, 8)), jnp.float32)
    return dict(prompt=prompt, gain_first=gain_first, gate_first=gate_first, up_first=up_first, down_first=down_first, gain_second=gain_second, gate_second=gate_second, up_second=up_second, down_second=down_second)


def normalize(rows):
    rows = rows.astype(jnp.float32)
    scale = jax.lax.rsqrt(lax.optimization_barrier(jnp.mean(rows * rows, axis=-1, keepdims=True)) + 1e-06)
    return (rows * scale).astype(jnp.bfloat16)

def layer_branch(normed, w_gate, w_up, w_down):
    gate = jnp.dot(normed, w_gate, preferred_element_type=jnp.float32)
    upper = jnp.dot(normed, w_up, preferred_element_type=jnp.float32)
    hidden = (jax.nn.silu(gate) * upper).astype(jnp.bfloat16)
    width = hidden.shape[1] // N_TP
    total = jnp.zeros((hidden.shape[0], w_down.shape[1]), jnp.float32)
    for block in range(N_TP):
        part = jnp.dot(hidden[:, block * width:(block + 1) * width], w_down[block * width:(block + 1) * width, :], preferred_element_type=jnp.float32)
        total = total + part.astype(jnp.bfloat16).astype(jnp.float32)
    return total

def reference(prompt, gain_first, gate_first, up_first, down_first, gain_second, gate_second, up_second, down_second):
    serve_gate_first = (gain_first[:, None] * gate_first).astype(jnp.bfloat16)
    serve_up_first = (gain_first[:, None] * up_first).astype(jnp.bfloat16)
    serve_down_first = down_first.astype(jnp.bfloat16)
    serve_gate_second = (gain_second[:, None] * gate_second).astype(jnp.bfloat16)
    serve_up_second = (gain_second[:, None] * up_second).astype(jnp.bfloat16)
    serve_down_second = down_second.astype(jnp.bfloat16)
    stream = prompt.astype(jnp.float32) + 0.5 * layer_branch(normalize(prompt), serve_gate_first, serve_up_first, serve_down_first)
    mixed = (stream + 0.5 * layer_branch(normalize(stream), serve_gate_second, serve_up_second, serve_down_second)).astype(jnp.bfloat16)
    return (serve_gate_first, serve_up_first, serve_down_first, serve_gate_second, serve_up_second, serve_down_second, mixed)
```

```python
import functools
import heapq

import jax
import jax.numpy as jnp
from jax import lax
from jax.experimental import pallas as pl
from jax.experimental.pallas import tpu as pltpu
from jax.sharding import PartitionSpec as P

MESH = pl.DeviceIdType.MESH
F32, BF16 = jnp.float32, jnp.bfloat16
NX, NY, NZ = 4, 4, 8
CHUNKS = 4

UNIT = 1.05
WIRE = 1.9
DOWN = 2.1
ROWS = 5.7
PAIR = 0.5


class Copy:
    def __init__(self, name, link, dur, **at):
        self.name, self.link, self.dur, self.at = name, link, dur, at
        self.idx = None


class Plan:
    def __init__(self):
        self.copies, self.tasks = {}, {}

    def copy(self, name, link, dur, late=0.0, **at):
        c = Copy(name, link, dur, **at)
        c.idx, c.late = len(self.copies), late
        self.copies[name] = c
        return c

    def task(self, name, needs, dur, sends=(), rank=0):
        self.tasks[name] = (set(needs), dur, list(sends), rank)

    def order(self):
        users = {}
        left = {}
        for name, (needs, *_) in self.tasks.items():
            left[name] = set(needs)
            for n in needs:
                users.setdefault(n, []).append(name)
        free, ready, coming, seq, now = {}, [], [], 0, 0.0
        for pos, name in enumerate(self.tasks):
            if not left[name]:
                heapq.heappush(ready, (self.tasks[name][3], pos, name))
        place = {name: pos for pos, name in enumerate(self.tasks)}
        done, times = [], {}

        def happened(event, at):
            times[event] = at
            for name in users.get(event, ()):
                left[name].discard(event)
                if not left[name]:
                    heapq.heappush(ready, (self.tasks[name][3], place[name] if self.tasks[name][3] else at, name))

        while ready or coming:
            while coming and (coming[0][0] <= now or not ready):
                at, _, event = heapq.heappop(coming)
                now = max(now, at)
                happened(event, at)
            if not ready:
                continue
            _, _, name = heapq.heappop(ready)
            _, dur, sends, _ = self.tasks[name]
            now += dur
            done.append(name)
            for c in sends:
                c = self.copies[c]
                end = max(now, free.get(c.link, 0.0)) + c.dur
                free[c.link] = end
                wire = 0.9 if c.link == "pair" else WIRE
                seq += 1
                heapq.heappush(coming, (end + wire + c.late, seq, c.name))
            happened(name, now)
        if len(done) != len(self.tasks):
            raise ValueError("plan stuck")
        self.times, self.total = times, now
        return done


def flip(link):
    return link[0] + ("-" if link[1] == "+" else "+")


def build_plan():
    p = Plan()
    whole = {0: [], 1: []}
    down_all = {0: [], 1: []}

    for l in (0, 1):
        after = ["begin"] if l == 0 else ["next"]
        g, u = f"G{l}", f"U{l}"
        have = whole[l]

        def put(buf, link, zrel, xrel, half, tag, have=have):
            dur = UNIT * (0.5 if half is not None else 1.0)
            c = p.copy(f"{buf}:{tag}", link, dur, buf=buf, z=zrel, x=xrel, half=half)
            have.append(c.name)
            return c.name

        first = []
        chain = []
        for s in ("+", "-"):
            sign = -1 if s == "+" else 1
            first.append(put(g, "z" + s, sign, 0, None, f"z{s}1"))
        for s in ("+", "-"):
            sign = -1 if s == "+" else 1
            first.append(put(u, "x" + s, 0, sign, None, f"x{s}"))
        for s in ("+", "-"):
            sign = -1 if s == "+" else 1
            first.append(put(u, "z" + s, sign, 0, None, f"o:z{s}1"))
        for s in ("+", "-"):
            sign = -1 if s == "+" else 1
            first.append(put(g, "x" + s, 0, sign, None, f"own:x{s}"))
        p.task(f"start{l}", after, 0.3, first)

        for s in ("+", "-"):
            sign = -1 if s == "+" else 1
            half = 0 if s == "+" else 1
            p.task(f"{g}fwd:own{s}", [f"{g}:own:x{s}"], 0.03, [put(g, "x" + s, 0, 2, half, f"own:xx{s}")])
            for step in (1, 2, 3, 4):
                src = f"{g}:z{s}{step}"
                zrel = sign * step
                h = half if step == 4 else None
                sends = []
                if step < 4:
                    nh = half if step == 3 else None
                    sends.append(put(g, "z" + s, sign * (step + 1), 0, nh, f"z{s}{step + 1}"))
                for t in ("+", "-"):
                    sends.append(put(g, "x" + t, zrel, -1 if t == "+" else 1, h, f"z{s}{step}:x{t}"))
                p.task(f"{g}fwd:z{s}{step}", [src], 0.03, sends)
                p.task(
                    f"{g}fwd:z{s}{step}x",
                    [f"{g}:z{s}{step}:x{s}"],
                    0.03,
                    [put(g, "x" + s, zrel, 2, h, f"z{s}{step}:xx")],
                )
        for s in ("+", "-"):
            sign = -1 if s == "+" else 1
            half = 0 if s == "+" else 1
            sends = [put(u, "x" + s, 0, 2, half, f"xx{s}")]
            name = "l" if s == "+" else "r"
            for t in ("+", "-"):
                sends.append(put(u, "z" + t, -1 if t == "+" else 1, sign, None, f"{name}:z{t}1"))
            p.task(f"{u}fwd:x{s}", [f"{u}:x{s}"], 0.03, sends)
        sends = [put(u, "z" + t, -1 if t == "+" else 1, 2, None, f"f:z{t}1") for t in ("+", "-")]
        p.task(f"{u}fwd:xx", [f"{u}:xx+", f"{u}:xx-"], 0.03, sends)
        for name, xrel in (("o", 0), ("l", -1), ("r", 1), ("f", 2)):
            for t in ("+", "-"):
                sign = -1 if t == "+" else 1
                last = 4 if (t == "+") == (name in ("o", "r")) else 3
                for step in range(1, last):
                    c = put(u, "z" + t, sign * (step + 1), xrel, None, f"{name}:z{t}{step + 1}")
                    p.task(f"{u}fwd:{name}:z{t}{step}", [f"{u}:{name}:z{t}{step}"], 0.03, [c])

        d = f"D{l}"
        p.copy(f"{d}:own", "y+", 2.0, late=4.0, buf=d, kind="own")
        for k in range(CHUNKS):
            down_all[l].append(p.copy(f"{d}:z+{k}", "z+", DOWN, late=9.0, buf=d, kind="z", chunk=k).name)
            p.copy(f"{d}:z-{k}", "z-", DOWN, buf=d, kind="z", chunk=k)
            for s in ("+", "-"):
                down_all[l].append(
                    p.copy(f"{d}:x{s}{k}", "x" + s, DOWN, buf=d, kind="x", chunk=k, x=-1 if s == "+" else 1).name
                )
            s = "+" if k % 2 == 0 else "-"
            down_all[l].append(p.copy(f"{d}:xx{k}", "x" + s, DOWN, buf=d, kind="x", chunk=k, x=2).name)
            p.task(f"{d}fwd:x{k}", [f"{d}:x{s}{k}"], 0.03, [f"{d}:xx{k}"])
            p.task(f"{d}hop{k}", [f"{d}:z+{k}"], 0.05, [f"{d}:x+{k}", f"{d}:x-{k}"])
        p.task(
            f"{d}src",
            [f"{d}:own", f"U{l}:l:z+2"],
            0.1,
            [f"{d}:z{s}{k}" for k in range(CHUNKS) for s in ("+", "-")],
        )

    p.task("begin", [], 1.0, ["D0:own", "D1:own"])
    p.task("next", ["start0", "D0src", "U0:f:z+2"], 0.02)
    p.task("norm1", ["start0"], 2.0, rank=1)
    p.task("h1", ["norm1"] + whole[0], 3.0, rank=1)
    p.task("asm1", down_all[0], 0.8, rank=1)
    reduce_tasks(p, 0, ["h1", "asm1"], {r: [] for r in range(4)})
    p.copy("N:y+", "y+", ROWS, buf="N", y=-1, half=None, core=0)
    p.copy("N:y-", "y-", ROWS, buf="N", y=1, half=None, core=0)
    p.copy("N:yy+", "y+", ROWS / 2, buf="N", y=2, half=0, core=0)
    p.copy("N:yy-", "y-", ROWS / 2, buf="N", y=2, half=1, core=0)
    p.copy("N:p0", "pair", PAIR, buf="N", y=0, half=None, core=1)
    p.copy("N:p-", "pair", PAIR, buf="N", y=-1, half=None, core=1)
    p.copy("N:p+", "pair", PAIR, buf="N", y=1, half=None, core=1)
    p.copy("N:q0", "pair", PAIR / 2, buf="N", y=2, half=0, core=1)
    p.copy("N:q1", "pair", PAIR / 2, buf="N", y=2, half=1, core=1)
    p.tasks["final0"][2].extend(["N:y+", "N:y-", "N:p0"])
    p.task("Nfwd:+", ["N:y+"], 0.03, ["N:yy+", "N:p-"])
    p.task("Nfwd:-", ["N:y-"], 0.03, ["N:yy-", "N:p+"])
    p.task("Nfwd:h0", ["N:yy+"], 0.03, ["N:q0"])
    p.task("Nfwd:h1", ["N:yy-"], 0.03, ["N:q1"])
    rows = {
        0: ["final0", "N:p0"],
        3: ["N:y+", "N:p-"],
        1: ["N:y-", "N:p+"],
        2: ["N:yy+", "N:yy-", "N:q0", "N:q1"],
    }
    for r in (0, 3, 1, 2):
        p.task(f"h2:{r}", rows[r] + whole[1], 1.3, rank=1)
    p.task("asm2", down_all[1], 0.8, rank=1)
    reduce_tasks(p, 1, ["asm2"], {r: [f"h2:{r}"] for r in range(4)})
    for l in (0, 1):
        p.whole, p.down_all = whole, down_all
    p.sequence = p.order()
    return p


def reduce_tasks(p, l, needs, per):
    for r in (2, 1, 3, 0):
        p.copy(f"R{l}:pair{r}", "pair", PAIR, buf=f"R{l}", kind="pair", rel=r)
        p.task(f"part{l}:{r}", needs + per[r], 0.8, [f"R{l}:pair{r}"], rank=1)
    p.copy(f"R{l}:far+", "y+", ROWS / 2, buf=f"R{l}", kind="far", side=0)
    p.copy(f"R{l}:far-", "y-", ROWS / 2, buf=f"R{l}", kind="far", side=1)
    p.copy(f"R{l}:near+", "y+", ROWS, buf=f"R{l}", kind="near", side=0)
    p.copy(f"R{l}:near-", "y-", ROWS, buf=f"R{l}", kind="near", side=1)
    p.task(f"sum{l}:2", [f"part{l}:2", f"R{l}:pair2"], 0.2, [f"R{l}:far+", f"R{l}:far-"])
    p.task(f"sum{l}:1", [f"part{l}:1", f"R{l}:pair1", f"R{l}:far+"], 0.2, [f"R{l}:near+"])
    p.task(f"sum{l}:3", [f"part{l}:3", f"R{l}:pair3", f"R{l}:far-"], 0.2, [f"R{l}:near-"])
    p.task(f"final{l}", [f"part{l}:0", f"R{l}:pair0", f"R{l}:near+", f"R{l}:near-"], 0.6)


def normalized(rows):
    scale = lax.rsqrt(jnp.mean(rows * rows, axis=-1, keepdims=True) + 1e-06)
    return (rows * scale).astype(BF16)


def gated(normed, w_gate, w_up):
    gate = jnp.dot(normed, w_gate, preferred_element_type=F32)
    upper = jnp.dot(normed, w_up, preferred_element_type=F32)
    return (gate / (1.0 + jnp.exp(-gate)) * upper).astype(BF16)


def kernel(
    plan,
    prompt_hbm,
    gain_a, gate_a, up_a, down_a,
    gain_b, gate_b, up_b, down_b,
    g0, u0, t0, g1, u1, t1, mixed,
    prompt, normed, hidden, part, stream,
    d0, d1, stage, pair0, pair1, far0, far1, near0, near1, sums,
    load_sem, send_sem, recv_sem, own_sem,
):
    gr, fs, tp = lax.axis_index("gr"), lax.axis_index("fs"), lax.axis_index("tp")
    z = gr * 4 + fs // 4
    x = lax.rem(fs, 4)
    y = tp // 2
    core = lax.rem(tp, 2)

    def device(xx, yy, zz, cc):
        return (zz // 4, lax.rem(zz, 4) * 4 + xx, yy * 2 + cc)

    def zat(k):
        return lax.rem(z + (k % NZ), NZ) if k % NZ else z

    def xat(k):
        return lax.rem(x + (k % NX), NX) if k % NX else x

    def yat(k):
        return lax.rem(y + (k % NY), NY) if k % NY else y

    other = 1 - core
    peers = {
        "z+": device(x, y, zat(1), core),
        "z-": device(x, y, zat(-1), core),
        "x+": device(xat(1), y, z, core),
        "x-": device(xat(-1), y, z, core),
        "y+": device(x, yat(1), z, core),
        "y-": device(x, yat(-1), z, core),
        "pair": device(x, y, z, other),
    }
    steps = {"z+": (1, 0, 0), "z-": (-1, 0, 0), "x+": (0, 1, 0), "x-": (0, -1, 0), "y+": (0, 0, 1), "y-": (0, 0, -1), "pair": (0, 0, 0)}
    weights = {"G0": g0, "U0": u0, "G1": g1, "U1": u1}
    downs = {"D0": d0, "D1": d1}
    pairs, fars, nears = (pair0, pair1), (far0, far1), (near0, near1)
    dist = lax.rem(z + NZ - tp, NZ)

    def refs(c, sender):
        dz, dx, dy = steps[c.link] if sender else (0, 0, 0)
        at = c.at
        buf = at["buf"]
        if buf in weights:
            row = (zat(at["z"] + dz) * NX + xat(at["x"] + dx)) * 64
            size = 64
            if at["half"] is not None:
                row, size = row + 32 * at["half"], 32
            ref = weights[buf].at[pl.ds(pl.multiple_of(row, 32), size), :]
            return ref, ref
        if buf in downs:
            n = 8 // CHUNKS
            xx = xat(at.get("x", 0) + dx)
            ref = downs[buf].at[xx, pl.ds(at["chunk"] * n, n)]
            return ref, ref
        if buf == "N":
            cc = core if (at["core"] == 0) == (True) else None
            if at["core"] == 1:
                cc = core if sender else other
            row = (yat(at["y"] + dy) * 2 + cc) * 64
            size = 64
            if at["half"] is not None:
                row, size = row + 32 * at["half"], 32
            ref = normed.at[pl.ds(pl.multiple_of(row, 32), size), :]
            return ref, ref
        l = int(buf[1])
        if at["kind"] == "pair":
            row = (yat(at["rel"]) * 2 + other) * 64
            return part.at[l, pl.ds(pl.multiple_of(row, 64), 64), :], pairs[l].at[at["rel"]]
        if at["kind"] == "far":
            s = at["side"]
            return sums.at[l, 2, pl.ds(32 * s, 32), :], fars[l].at[s]
        s = at["side"]
        return sums.at[l, 1 if s == 0 else 3], nears[l].at[s]

    def describe(c, sender):
        src, dst = refs(c, sender)
        return pltpu.make_async_remote_copy(
            src_ref=src,
            dst_ref=dst,
            send_sem=send_sem.at[c.idx],
            recv_sem=recv_sem.at[c.idx],
            device_id=peers[c.link],
            device_id_type=MESH,
        )

    def own_copy(l):
        return pltpu.make_async_remote_copy(
            src_ref=stage.at[l],
            dst_ref=downs[f"D{l}"].at[x, tp],
            send_sem=send_sem.at[plan.copies[f"D{l}:own"].idx],
            recv_sem=own_sem.at[l, tp],
            device_id=device(x, z // 2, z, lax.rem(z, 2)),
            device_id_type=MESH,
        )

    def down_sends(c, first=None):
        here = dist == 0
        if c.link == "z+":
            later = jnp.logical_and(dist > 0, dist < 4)
        else:
            later = dist > 5
        if first is None:
            return jnp.logical_or(here, later)
        return here if first else later

    def send(name, first=False):
        c = plan.copies[name]
        if c.at["buf"] in downs:
            if c.at["kind"] == "own":
                l = int(c.at["buf"][1])

                @pl.when(tp != z)
                def _():
                    own_copy(l).start()

                return
            if c.at["kind"] == "z":

                @pl.when(down_sends(c, first))
                def _():
                    describe(c, True).start()

                return
        describe(c, True).start()

    def sent(c):
        if c.at["buf"] in downs:
            if c.at["kind"] == "own":

                @pl.when(tp != z)
                def _():
                    own_copy(int(c.at["buf"][1])).wait_send()

                return
            if c.at["kind"] == "z":

                @pl.when(down_sends(c))
                def _():
                    describe(c, True).wait_send()

                return
        describe(c, True).wait_send()

    seen = set()

    def arrived(name):
        if name in seen or name not in plan.copies:
            return
        seen.add(name)
        c = plan.copies[name]
        if c.at["buf"] in downs and c.at["kind"] in ("own", "z"):
            if c.at["kind"] == "own":
                l = int(c.at["buf"][1])
                for t in range(8):

                    @pl.when(jnp.logical_and(dist == 0, tp != t))
                    def _(t=t):
                        pltpu.make_async_remote_copy(
                            src_ref=stage.at[l],
                            dst_ref=downs[c.at["buf"]].at[x, t],
                            send_sem=send_sem.at[c.idx],
                            recv_sem=own_sem.at[l, t],
                            device_id=peers["pair"],
                            device_id_type=MESH,
                        ).wait_recv()

                return
            back = plan.copies[name.replace("z+", "z-")]

            @pl.when(jnp.logical_and(dist > 0, dist < 5))
            def _():
                describe(c, False).wait_recv()

            @pl.when(dist > 4)
            def _():
                describe(back, False).wait_recv()

            return
        describe(c, False).wait_recv()

    eye = lax.broadcasted_iota(jnp.int32, (64, 64), 0) == lax.broadcasted_iota(jnp.int32, (64, 64), 1)

    def fold(gain, w):
        column = jnp.sum(jnp.where(eye, gain[...], 0.0), axis=1, keepdims=True)
        return (column * w[...]).astype(BF16)

    mine = pl.ds(pl.multiple_of((z * NX + x) * 64, 64), 64)

    def rows_of(r):
        return pl.ds(pl.multiple_of(yat(r) * 128, 128), 128)

    def block_of(r, cc):
        return pl.ds(pl.multiple_of((yat(r) * 2 + cc) * 64, 64), 64)

    load = pltpu.make_async_copy(prompt_hbm, prompt, load_sem)

    def begin():
        load.start()
        barrier = pltpu.get_barrier_semaphore()
        greet = [peers[k] for k in ("z+", "z-", "x+", "x-")]
        greet += [(gr, fs, lax.rem(tp + k, 8)) for k in range(1, 8)]
        for who in greet:
            pl.semaphore_signal(barrier, inc=1, device_id=who, device_id_type=MESH)
        g0[mine, :] = fold(gain_a, gate_a)
        u0[mine, :] = fold(gain_a, up_a)
        g1[mine, :] = fold(gain_b, gate_b)
        u1[mine, :] = fold(gain_b, up_b)
        for l, (src, dst) in enumerate(((down_a, d0), (down_b, d1))):
            stage[l] = src[...].astype(BF16)

            @pl.when(tp == z)
            def _(src=src, dst=dst):
                dst[x, tp] = src[...].astype(BF16)

        pl.semaphore_wait(barrier, len(greet))

    def norm1():
        load.wait()

        @pl.loop(0, 8)
        def _(i):
            at = pl.ds(pl.multiple_of(i * 64, 64), 64)
            normed[at, :] = normalized(prompt[at, :].astype(F32))

    def h1():
        @pl.loop(0, 2)
        def _(i):
            at = pl.ds(pl.multiple_of(i * 256, 256), 256)
            hidden[at, :] = gated(normed[at, :], g0[...], u0[...])

    def h2(r):
        at = rows_of(r)
        hidden[at, :] = gated(normed[at, :], g1[...], u1[...])

    def assemble(src, dst):
        for t in range(8):
            rows = jnp.concatenate([src[k, t].astype(F32) for k in range(NX)], axis=0)
            dst[:, 256 * t : 256 * (t + 1)] = rows.astype(BF16)

    def partial(l, r):
        at = rows_of(r)
        w = (t0, t1)[l]
        part[l, at, :] = jnp.dot(hidden[at, :], w[...], preferred_element_type=F32).astype(BF16)

    def chip_sum(l, r):
        return part[l, block_of(r, core), :].astype(F32) + pairs[l][r].astype(F32)

    def add_up(l, r):
        total = chip_sum(l, r)
        if r == 2:
            sums[l, 2] = total.astype(BF16)
            return
        side = 0 if r == 1 else 1
        at, rest = (slice(0, 32), slice(32, 64)) if side == 0 else (slice(32, 64), slice(0, 32))
        sums[l, r, at, :] = (total[at] + fars[l][side].astype(F32)).astype(BF16)
        sums[l, r, rest, :] = total[rest].astype(BF16)

    def final(l):
        total = chip_sum(l, 0) + nears[l][0].astype(F32) + nears[l][1].astype(F32)
        if l == 0:
            at = block_of(0, core)
            rows = prompt[at, :].astype(F32) + 0.5 * total
            stream[...] = rows
            normed[at, :] = normalized(rows)
        else:
            mixed[...] = (stream[...] + 0.5 * total).astype(BF16)

    for name in plan.sequence:
        needs, _, sends, _ = plan.tasks[name]
        for n in plan.copies:
            if n in needs:
                arrived(n)
        with jax.named_scope(name.split(":")[0]):
            if name == "begin":
                begin()
            elif name == "norm1":
                norm1()
            elif name == "h1":
                h1()
            elif name.startswith("h2:"):
                h2(int(name[3]))
            elif name == "asm1":
                assemble(d0, t0)
            elif name == "asm2":
                assemble(d1, t1)
            elif name.startswith("part"):
                partial(int(name[4]), int(name[6]))
            elif name.startswith("sum"):
                add_up(int(name[3]), int(name[5]))
            elif name.startswith("final"):
                final(int(name[5]))
        if name[2:5] == "hop":
            send(f"{name[:2]}:z+{name[5:]}")
            send(f"{name[:2]}:z-{name[5:]}")
        for n in sends:
            send(n, name[2:5] == "src")
    for c in plan.copies.values():
        sent(c)


def shards(prompt, gain_first, gate_first, up_first, down_first, gain_second, gate_second, up_second, down_second):
    plan = build_plan()
    rows, width = prompt.shape
    units = gate_first.shape[1]
    depth, columns = down_first.shape
    count = len(plan.copies)
    vmem = pl.BlockSpec(memory_space=pltpu.VMEM)
    gate_shape = jax.ShapeDtypeStruct((width, units), BF16)
    down_shape = jax.ShapeDtypeStruct((units, width), BF16)
    sem = pltpu.SemaphoreType.DMA
    block = rows // 8
    outs = pl.pallas_call(
        functools.partial(kernel, plan),
        out_shape=(gate_shape, gate_shape, down_shape, gate_shape, gate_shape, down_shape, jax.ShapeDtypeStruct((block, width), BF16)),
        in_specs=[pl.BlockSpec(memory_space=pl.ANY)] + [vmem] * 8,
        out_specs=(vmem,) * 7,
        scratch_shapes=[
            pltpu.VMEM((rows, width), BF16),
            pltpu.VMEM((rows, width), BF16),
            pltpu.VMEM((rows, units), BF16),
            pltpu.VMEM((2, rows, width), BF16),
            pltpu.VMEM((block, width), F32),
            pltpu.VMEM((NX, 8, depth, columns), BF16),
            pltpu.VMEM((NX, 8, depth, columns), BF16),
            pltpu.VMEM((2, depth, columns), BF16),
            pltpu.VMEM((NY, block, width), BF16),
            pltpu.VMEM((NY, block, width), BF16),
            pltpu.VMEM((2, block // 2, width), BF16),
            pltpu.VMEM((2, block // 2, width), BF16),
            pltpu.VMEM((2, block, width), BF16),
            pltpu.VMEM((2, block, width), BF16),
            pltpu.VMEM((2, NY, block, width), BF16),
            sem,
            sem((count,)),
            sem((count,)),
            sem((2, 8)),
        ],
        compiler_params=pltpu.CompilerParams(collective_id=0, has_side_effects=True, vmem_limit_bytes=48 * 1024 * 1024),
        name="handover",
    )(
        prompt,
        gain_first.reshape(1, -1), gate_first, up_first, down_first,
        gain_second.reshape(1, -1), gate_second, up_second, down_second,
    )
    return outs


def solution(mesh):
    rows = P(("gr", "fs"), None)
    block = P(("gr", "fs"), "tp")
    line = P(("gr", "fs"))
    return jax.shard_map(
        shards,
        mesh=mesh,
        in_specs=(rows, line, block, block, block, line, block, block, block),
        out_specs=(
            P(None, "tp"),
            P(None, "tp"),
            P("tp", None),
            P(None, "tp"),
            P(None, "tp"),
            P("tp", None),
            P(("gr", "fs", "tp"), None),
        ),
        check_vma=False,
    )
```

```python
import functools
import heapq

import jax
import jax.numpy as jnp
from jax import lax
from jax.experimental import pallas as pl
from jax.experimental.pallas import tpu as pltpu
from jax.sharding import PartitionSpec as P

MESH = pl.DeviceIdType.MESH
F32, BF16 = jnp.float32, jnp.bfloat16
NX, NY, NZ = 4, 4, 8
CHUNKS = 4

UNIT, DOWN, ROWS, PAIR, WIRE, NEAR = 1.08, 2.15, 5.7, 0.5, 2.0, 1.0

ZP, ZM, XP, XM, YP, YM, PR = LINKS = range(7)
STEP = {ZP: (1, 0, 0), ZM: (-1, 0, 0), XP: (0, 1, 0), XM: (0, -1, 0), YP: (0, 0, 1), YM: (0, 0, -1), PR: (0, 0, 0)}
G, U, D, N, R = range(5)
BEGIN, START, NORM, HIDE, GLUE, TURN, PART, SUM, LAST, SOURCE, PASS = range(100, 111)
OWN, ALONG, ACROSS, PAIRED, FAR, CLOSE = range(200, 206)


class Copy:
    def __init__(self, idx, link, dur, at):
        self.idx, self.link, self.dur = idx, link, dur
        self.buf = at["buf"]
        self.at = at


class Task:
    def __init__(self, needs, dur, sends, rank, only):
        self.needs, self.dur, self.sends, self.rank, self.only = list(needs), dur, list(sends), rank, only

    def falls_to(self, d):
        return self.only is None or min(d, NZ - d) == self.only


class Plan:
    def __init__(self):
        self.copies, self.tasks = {}, {}

    def copy(self, key, link, dur, **at):
        self.copies[key] = Copy(len(self.copies), link, dur, at)
        return key

    def task(self, key, needs, dur, sends=(), rank=0, only=None):
        self.tasks[key] = Task(needs, dur, sends, rank, only)

    def issues(self, key, d):
        for c in self.tasks[key].sends:
            copy = self.copies[c]
            if copy.buf == D and copy.at["kind"] == ALONG and not goes_on(copy.link, d):
                continue
            yield c, copy

    def absent(self, need, d):
        if need in self.tasks:
            return not self.tasks[need].falls_to(d)
        copy = self.copies.get(need)
        if copy is None or copy.buf != D:
            return False
        if copy.at["kind"] == OWN:
            return d != 0
        return copy.at["kind"] == ALONG and (d == 0 or (copy.link == ZP) != (d < 5))

    def simulate(self, fixed=None):
        kinds = [(d, c) for d in range(NZ) for c in range(2)]
        left = {k: {t: {n for n in v.needs if not self.absent(n, k[0])} for t, v in self.tasks.items() if v.falls_to(k[0])} for k in kinds}
        users = {}
        for t, v in self.tasks.items():
            for n in v.needs:
                users.setdefault(n, []).append(t)
        place = {t: i for i, t in enumerate(fixed or self.tasks)}
        ready = {k: [] for k in kinds}
        free = {}
        busy = {k: 0.0 for k in kinds}
        done = {k: {} for k in kinds}
        turn = {k: 0 for k in kinds}
        events, seq = [], 0

        def settle(k, need, at):
            done[k].setdefault(need, at)
            for t in users.get(need, ()):
                if need in left[k].get(t, ()):
                    left[k][t].discard(need)
                    if not left[k][t]:
                        heapq.heappush(ready[k], (self.tasks[t].rank, place[t] if self.tasks[t].rank else at, place[t], t))

        for k in kinds:
            for t in left[k]:
                if not left[k][t]:
                    heapq.heappush(ready[k], (self.tasks[t].rank, 0.0, place[t], t))
            heapq.heappush(events, (0.0, seq, k, None))
            seq += 1
        starts = {k: {} for k in kinds}
        while events:
            now, _, k, what = heapq.heappop(events)
            if what is not None:
                settle(k, what, now)
            if now < busy[k]:
                continue
            if fixed is None:
                if not ready[k]:
                    continue
                t = heapq.heappop(ready[k])[3]
            else:
                while turn[k] < len(fixed) and fixed[turn[k]] not in left[k]:
                    turn[k] += 1
                if turn[k] == len(fixed) or left[k][fixed[turn[k]]]:
                    continue
                t = fixed[turn[k]]
                turn[k] += 1
            starts[k][t] = now
            end = now + self.tasks[t].dur
            busy[k] = end
            d, c = k
            for name, copy in self.issues(t, d):
                at = max(end, free.get((k, copy.link), 0.0)) + copy.dur
                free[k, copy.link] = at
                dz, _, dy = STEP[copy.link]
                to = ((d + dz - 2 * dy) % NZ, c)
                if copy.buf == D and copy.at["kind"] == OWN:
                    to = (0, c)
                if copy.link == PR:
                    to = ((d + (-1 if c == 0 else 1)) % NZ, 1 - c)
                seq += 1
                heapq.heappush(events, (at + (NEAR if copy.link == PR else WIRE), seq, to, name))
            seq += 1
            heapq.heappush(events, (end, seq, k, t))
        return starts, max(busy.values())

    def line_up(self, starts, mix):
        at = {}
        for t in self.tasks:
            here = [v[t] for v in starts.values() if t in v]
            at[t] = mix * max(here) + (1 - mix) * sum(here) / len(here)
        place = {t: i for i, t in enumerate(self.tasks)}
        changed = True
        while changed:
            changed = False
            for t, before in self.before.items():
                for n in before:
                    if at[n] >= at[t]:
                        at[t] = at[n] + 1e-6
                        changed = True
        return sorted(self.tasks, key=lambda t: (at[t], place[t]))

    def find_before(self):
        starters, self.before = {}, {}
        for t, v in self.tasks.items():
            for c in v.sends:
                starters.setdefault(c, []).append(t)
        for t, v in self.tasks.items():
            before = [n for n in v.needs if n in self.tasks]
            for n in v.needs:
                for y in starters.get(n, ()):
                    hop = self.copies[n].buf == D and self.copies[n].at["kind"] == ALONG
                    m = self.tasks[y].only
                    if m is None or v.only is None or m == v.only - hop:
                        before.append(y)
            self.before[t] = before

    def order(self):
        self.find_before()
        starts, self.ideal = self.simulate()
        best = None
        for mix in (0.0, 0.2, 0.4, 0.6, 0.8, 1.0):
            line = self.line_up(starts, mix)
            total = self.simulate(line)[1]
            if best is None or total < best[0]:
                best = total, line
        self.total = best[0]
        return best[1]


def goes_on(link, d):
    return d < 4 if link == ZP else d == 0 or d > 5


RELEASE = [1, 2, 3, 0, 5, 2, 2, 7]


def mark(l, place):
    if place == 0:
        return (START, l)
    if place < 5:
        return (PASS, G, l, ALONG, 0, place)
    if place < 7:
        return (PASS, U, l, ALONG, 0, 0, place - 4)
    if place < 9:
        return (PASS, U, l, ALONG, 3, 0, place - 6)
    return (PASS, D, l, ACROSS, place - 9, 4)


def build_plan():
    p = Plan()
    whole, downs = ([], []), ([], [])
    signs = ((0, -1), (1, 1))
    zs, xs = (ZP, ZM), (XP, XM)

    p.task((BEGIN,), [], 3.0, [p.copy((D, l, OWN), YP, 2.0, buf=D, layer=l, kind=OWN) for l in (0, 1)])
    for l in (0, 1):

        def put(buf, link, zrel, xrel, half, *tag):
            key = (buf, l, *tag)
            whole[l].append(p.copy(key, link, UNIT * (1.0 if half is None else 0.5), buf=buf, layer=l, z=zrel, x=xrel, half=half))
            return key

        first = [put(G, zs[s], sign, 0, None, ALONG, s, 1) for s, sign in signs]
        first += [put(U, xs[s], 0, sign, None, ACROSS, s) for s, sign in signs]
        first += [put(U, zs[s], sign, 0, None, ALONG, 0, s, 1) for s, sign in signs]
        first += [put(G, xs[s], 0, sign, None, OWN, s) for s, sign in signs]
        p.task((START, l), [(BEGIN,)] if l == 0 else [mark(0, RELEASE[3 + CHUNKS])], 0.2, first)

        for s, sign in signs:
            p.task((PASS, G, l, OWN, s), [(G, l, OWN, s)], 0.03, [put(G, xs[s], 0, 2, s, OWN, s, 2)])
            for step in (1, 2, 3, 4):
                zrel, half = sign * step, s if step == 4 else None
                sends = []
                if step < 4:
                    sends.append(put(G, zs[s], sign * (step + 1), 0, s if step == 3 else None, ALONG, s, step + 1))
                for t, to in signs:
                    sends.append(put(G, xs[t], zrel, to, half, ACROSS, s, step, t))
                p.task((PASS, G, l, ALONG, s, step), [(G, l, ALONG, s, step)], 0.03, sends)
                p.task((PASS, G, l, ACROSS, s, step), [(G, l, ACROSS, s, step, s)], 0.03, [put(G, xs[s], zrel, 2, half, ACROSS, s, step, 2)])
        for s, sign in signs:
            p.task((PASS, U, l, ACROSS, s), [(U, l, ACROSS, s)], 0.03, [put(U, xs[s], 0, 2, s, ACROSS, s, 2)])
            sends = [put(U, zs[t], to, sign, None, ALONG, 1 + s, t, 1) for t, to in signs]
            p.task((PASS, U, l, ALONG, 1 + s), [(U, l, ACROSS, s), mark(l, RELEASE[s])], 0.03, sends)
        sends = [put(U, zs[t], to, 2, None, ALONG, 3, t, 1) for t, to in signs]
        p.task((PASS, U, l, ALONG, 3), [(U, l, ACROSS, 0, 2), (U, l, ACROSS, 1, 2), mark(l, RELEASE[2])], 0.03, sends)
        for column, xrel in enumerate((0, -1, 1, 2)):
            for t, sign in signs:
                for step in range(1, 4 if (t == 0) == (column in (0, 2)) else 3):
                    c = put(U, zs[t], sign * (step + 1), xrel, None, ALONG, column, t, step + 1)
                    p.task((PASS, U, l, ALONG, column, t, step), [(U, l, ALONG, column, t, step)], 0.03, [c])

        along = {}
        for k in range(CHUNKS):
            for s, sign in signs:
                along[k, s] = p.copy((D, l, ALONG, k, s), zs[s], DOWN, buf=D, layer=l, kind=ALONG, chunk=k)
            sends = [along[k, 0], along[k, 1]]
            sends += [p.copy((D, l, ACROSS, k, s), xs[s], DOWN, buf=D, layer=l, kind=ACROSS, chunk=k, x=sign) for s, sign in signs]
            s = k % 2
            c = p.copy((D, l, ACROSS, k, 2), xs[s], DOWN, buf=D, layer=l, kind=ACROSS, chunk=k, x=2)
            for m in range(NZ // 2 + 1):
                needs = [(SOURCE, l), mark(l, RELEASE[3 + k])] if m == 0 else [along[k, 0], along[k, 1]]
                p.task((PASS, D, l, ALONG, k, m), needs, 0.05, sends, only=m)
                p.task((PASS, D, l, ACROSS, k, m), [(D, l, ACROSS, k, s)], 0.03, [c], only=m)
                downs[l].append((PASS, D, l, ALONG, k, m))
            downs[l].extend([sends[2], sends[3], c])
        p.task((SOURCE, l), [(D, l, OWN)], 0.1, [], only=0)

    p.task((NORM,), [(START, 0)], 2.0, rank=1)
    p.task((HIDE, 0), [(NORM,)] + whole[0], 3.0, rank=1)
    p.task((GLUE, 0), downs[0], 0.8, rank=1)
    add_reduce(p, 0, [(HIDE, 0), (GLUE, 0)], {r: [] for r in range(4)})
    for s, sign in signs:
        c = p.copy((N, CLOSE, s), (YP, YM)[s], ROWS, buf=N, y=sign, half=None, core=0)
        p.tasks[LAST, 0].sends.append(c)
        far = p.copy((N, FAR, s), (YP, YM)[s], ROWS / 2, buf=N, y=2, half=s, core=0)
        near = p.copy((N, PAIRED, s), PR, PAIR, buf=N, y=sign, half=None, core=1)
        p.task((PASS, N, CLOSE, s), [c], 0.03, [far, near])
        p.task((PASS, N, FAR, s), [far], 0.03, [p.copy((N, PAIRED, FAR, s), PR, PAIR / 2, buf=N, y=2, half=s, core=1)])
    p.tasks[LAST, 0].sends.append(p.copy((N, PAIRED), PR, PAIR, buf=N, y=0, half=None, core=1))
    rows = {
        0: [(LAST, 0), (N, PAIRED)],
        3: [(N, CLOSE, 0), (N, PAIRED, 0)],
        1: [(N, CLOSE, 1), (N, PAIRED, 1)],
        2: [(N, FAR, 0), (N, FAR, 1), (N, PAIRED, FAR, 0), (N, PAIRED, FAR, 1)],
    }
    for r in (0, 3, 1, 2):
        p.task((HIDE, 1, r), rows[r] + whole[1], 1.3, rank=1)
    p.task((GLUE, 1), downs[1], 0.8, rank=1)
    add_reduce(p, 1, [(GLUE, 1)], {r: [(HIDE, 1, r)] for r in range(4)})
    for l in (0, 1):
        for buf in (G, U):
            for part in (0, 1):
                p.task((TURN, buf, l, part), whole[l] + [(HIDE, 0)], 0.5, rank=2)
    p.sequence = p.order()
    return p


def add_reduce(p, l, needs, per):
    for r in (2, 1, 3, 0):
        c = p.copy((R, l, PAIRED, r), PR, PAIR, buf=R, layer=l, kind=PAIRED, rel=r)
        p.task((PART, l, r), needs + per[r], 0.8, [c], rank=1)
    far = [p.copy((R, l, FAR, s), (YP, YM)[s], ROWS / 2, buf=R, layer=l, kind=FAR, side=s) for s in (0, 1)]
    near = [p.copy((R, l, CLOSE, s), (YP, YM)[s], ROWS, buf=R, layer=l, kind=CLOSE, side=s) for s in (0, 1)]
    p.task((SUM, l, 2), [(PART, l, 2), (R, l, PAIRED, 2)], 0.2, far)
    for s, r in enumerate((1, 3)):
        p.task((SUM, l, r), [(PART, l, r), (R, l, PAIRED, r), far[s]], 0.2, [near[s]])
    p.task((LAST, l), [(PART, l, 0), (R, l, PAIRED, 0)] + near, 0.6)


def normalized(rows):
    scale = lax.rsqrt(jnp.mean(rows * rows, axis=-1, keepdims=True) + 1e-06)
    return (rows * scale).astype(BF16)


def gated(normed, w_gate, w_up):
    gate = jnp.dot(normed, w_gate, preferred_element_type=F32)
    upper = jnp.dot(normed, w_up, preferred_element_type=F32)
    return (gate / (1.0 + jnp.exp(-gate)) * upper).astype(BF16)


def kernel(
    plan,
    prompt_hbm,
    gain_a, gate_a, up_a, down_a,
    gain_b, gate_b, up_b, down_b,
    gt0, ut0, t0, gt1, ut1, t1, mixed,
    prompt, normed, hidden, part, stream,
    g0, u0, g1, u1, d0, d1, stage,
    pair0, pair1, far0, far1, near0, near1, sums,
    gains, gates, depths,
    load_sem, send_sem, recv_sem, own_sem,
):
    gr, fs, tp = lax.axis_index("gr"), lax.axis_index("fs"), lax.axis_index("tp")
    z = gr * 4 + fs // 4
    x = lax.rem(fs, 4)
    y = tp // 2
    core = lax.rem(tp, 2)

    def device(xx, yy, zz, cc):
        return (zz // 4, lax.rem(zz, 4) * 4 + xx, yy * 2 + cc)

    def zat(k):
        return lax.rem(z + (k % NZ), NZ) if k % NZ else z

    def xat(k):
        return lax.rem(x + (k % NX), NX) if k % NX else x

    def yat(k):
        return lax.rem(y + (k % NY), NY) if k % NY else y

    other = 1 - core
    peers = {
        ZP: device(x, y, zat(1), core),
        ZM: device(x, y, zat(-1), core),
        XP: device(xat(1), y, z, core),
        XM: device(xat(-1), y, z, core),
        YP: device(x, yat(1), z, core),
        YM: device(x, yat(-1), z, core),
        PR: device(x, y, z, other),
    }
    weights = {(G, 0): g0, (U, 0): u0, (G, 1): g1, (U, 1): u1}
    turned = {(G, 0): gt0, (U, 0): ut0, (G, 1): gt1, (U, 1): ut1}
    downs, talls = (d0, d1), (t0, t1)
    pairs, fars, nears = (pair0, pair1), (far0, far1), (near0, near1)
    dist = lax.rem(z + NZ - tp, NZ)

    def rows_at(ref, row, half):
        if half is None:
            return ref.at[pl.ds(pl.multiple_of(row, 64), 64), :]
        return ref.at[pl.ds(pl.multiple_of(row + 32 * half, 32), 32), :]

    def refs(c, sender):
        dz, dx, dy = STEP[c.link] if sender else (0, 0, 0)
        at = c.at
        if c.buf in (G, U):
            row = (zat(at["z"] + dz) * NX + xat(at["x"] + dx)) * 64
            ref = rows_at(weights[c.buf, at["layer"]], row, at["half"])
            return ref, ref
        if c.buf == D:
            n = 8 // CHUNKS
            ref = downs[at["layer"]].at[xat(at.get("x", 0) + dx), pl.ds(at["chunk"] * n, n)]
            return ref, ref
        if c.buf == N:
            cc = other if at["core"] and not sender else core
            ref = rows_at(normed, (yat(at["y"] + dy) * 2 + cc) * 64, at["half"])
            return ref, ref
        l = at["layer"]
        if at["kind"] == PAIRED:
            return rows_at(part.at[l], (yat(at["rel"]) * 2 + other) * 64, None), pairs[l].at[at["rel"]]
        side = at["side"]
        if at["kind"] == FAR:
            return sums.at[l, 2, pl.ds(32 * side, 32), :], fars[l].at[side]
        return sums.at[l, 1 + 2 * side], nears[l].at[side]

    def describe(c, sender):
        src, dst = refs(c, sender)
        return pltpu.make_async_remote_copy(
            src_ref=src,
            dst_ref=dst,
            send_sem=send_sem.at[c.idx],
            recv_sem=recv_sem.at[c.idx],
            device_id=peers[c.link],
            device_id_type=MESH,
        )

    def own_copy(c, t):
        l = c.at["layer"]
        return pltpu.make_async_remote_copy(
            src_ref=stage.at[l],
            dst_ref=downs[l].at[x, t],
            send_sem=send_sem.at[c.idx],
            recv_sem=own_sem.at[l, t],
            device_id=device(x, z // 2, z, lax.rem(z, 2)),
            device_id_type=MESH,
        )

    def passes(c):
        if c.buf != D or c.at["kind"] == ACROSS:
            return None
        if c.at["kind"] == OWN:
            return dist != 0
        return dist < 4 if c.link == ZP else jnp.logical_or(dist == 0, dist > 5)

    def if_so(here, act):
        if here is None:
            act()
        else:
            pl.when(here)(act)

    def is_own(c):
        return c.buf == D and c.at["kind"] == OWN

    def send(c, here):
        copy = own_copy(c, tp) if is_own(c) else describe(c, True)
        if_so(here, copy.start)

    def sent(c):
        copy = own_copy(c, tp) if is_own(c) else describe(c, True)
        if_so(passes(c), copy.wait_send)

    seen = set()

    def arrived(key, only):
        c = plan.copies[key]
        if c.buf == D and c.at["kind"] == ALONG:
            if_so(dist == (only if c.link == ZP else NZ - only), describe(c, False).wait_recv)
            return
        if (key, only) in seen or (only is None and (key, 4) in seen):
            return
        seen.add((key, only))
        if is_own(c):
            for t in range(8):
                if_so(jnp.logical_and(dist == 0, tp != t), own_copy(c, t).wait_recv)
            return
        here = None if only is None else hops == only
        if_so(here, describe(c, False).wait_recv)

    hops = jnp.minimum(dist, NZ - dist)
    eye = lax.broadcasted_iota(jnp.int32, (64, 64), 0) == lax.broadcasted_iota(jnp.int32, (64, 64), 1)

    def fold(gain, w):
        column = jnp.sum(jnp.where(eye, gain[...], 0.0), axis=1, keepdims=True)
        return (column * w[...]).astype(BF16)

    mine = pl.ds(pl.multiple_of((z * NX + x) * 64, 64), 64)

    def rows_of(r):
        return pl.ds(pl.multiple_of(yat(r) * 128, 128), 128)

    def block_of(r, cc):
        return pl.ds(pl.multiple_of((yat(r) * 2 + cc) * 64, 64), 64)

    loads = [
        pltpu.make_async_copy(src, dst, load_sem.at[i])
        for i, (src, dst) in enumerate(
            (
                (gain_a, gains.at[0]), (gate_a, gates.at[0]), (up_a, gates.at[1]), (down_a, depths.at[0]),
                (gain_b, gains.at[1]), (gate_b, gates.at[2]), (up_b, gates.at[3]), (down_b, depths.at[1]),
                (prompt_hbm, prompt),
            )
        )
    ]

    def begin():
        for load in loads:
            load.start()
        barrier = pltpu.get_barrier_semaphore()
        greet = [peers[k] for k in (ZP, ZM, XP, XM)]
        greet += [(gr, fs, lax.rem(tp + k, 8)) for k in range(1, 8)]
        for who in greet:
            pl.semaphore_signal(barrier, inc=1, device_id=who, device_id_type=MESH)
        for load in loads[:8]:
            load.wait()
        for i, ref in enumerate((g0, u0, g1, u1)):
            ref[mine, :] = fold(gains.at[i // 2], gates.at[i])
        for l in (0, 1):
            stage[l] = depths[l].astype(BF16)

            @pl.when(dist == 0)
            def _(l=l):
                downs[l][x, tp] = depths[l].astype(BF16)

        pl.semaphore_wait(barrier, len(greet))

    def norm():
        loads[8].wait()

        @pl.loop(0, 8)
        def _(i):
            at = pl.ds(pl.multiple_of(i * 64, 64), 64)
            normed[at, :] = normalized(prompt[at, :].astype(F32))

    def hide(l, r=None):
        if l == 0:

            @pl.loop(0, 2)
            def _(i):
                at = pl.ds(pl.multiple_of(i * 256, 256), 256)
                hidden[at, :] = gated(normed[at, :], g0[...], u0[...])

        else:
            at = rows_of(r)
            hidden[at, :] = gated(normed[at, :], g1[...], u1[...])

    def turn(buf, l, piece):
        src, dst = weights[buf, l], turned[buf, l]

        @pl.loop(0, 4)
        def _(i):
            at = pl.ds(pl.multiple_of((piece * 4 + i) * 256, 256), 256)
            dst[:, at] = src[at, :].astype(F32).T.astype(BF16)

    def glue(l):
        for t in range(8):
            rows = jnp.concatenate([downs[l][k, t].astype(F32) for k in range(NX)], axis=0)
            talls[l][:, 256 * t : 256 * (t + 1)] = rows.astype(BF16)

    def partial(l, r):
        at = rows_of(r)
        part[l, at, :] = jnp.dot(hidden[at, :], talls[l][...], preferred_element_type=F32).astype(BF16)

    def chip_sum(l, r):
        return part[l, block_of(r, core), :].astype(F32) + pairs[l][r].astype(F32)

    def add_up(l, r):
        total = chip_sum(l, r)
        if r == 2:
            sums[l, 2] = total.astype(BF16)
            return
        side = 0 if r == 1 else 1
        at, rest = (slice(0, 32), slice(32, 64)) if side == 0 else (slice(32, 64), slice(0, 32))
        sums[l, r, at, :] = (total[at] + fars[l][side].astype(F32)).astype(BF16)
        sums[l, r, rest, :] = total[rest].astype(BF16)

    def last(l):
        total = chip_sum(l, 0) + nears[l][0].astype(F32) + nears[l][1].astype(F32)
        if l == 0:
            at = block_of(0, core)
            rows = prompt[at, :].astype(F32) + 0.5 * total
            stream[...] = rows
            normed[at, :] = normalized(rows)
        else:
            mixed[...] = (stream[...] + 0.5 * total).astype(BF16)

    work = {BEGIN: begin, NORM: norm, HIDE: hide, TURN: turn, GLUE: glue, PART: partial, SUM: add_up, LAST: last}
    for key in plan.sequence:
        task = plan.tasks[key]
        for n in task.needs:
            if n in plan.copies and not (task.only == 4 and plan.copies[n].link == ZM and plan.copies[n].at.get("kind") == ALONG):
                arrived(n, task.only)
        if key[0] in work:
            work[key[0]](*key[1:])
        for n in task.sends:
            c = plan.copies[n]
            here = passes(c)
            if task.only is not None:
                here = hops == task.only if here is None else jnp.logical_and(here, hops == task.only)
            send(c, here)
    for c in plan.copies.values():
        sent(c)


def hand_out(*refs):
    sources, targets, sem = refs[:7], refs[7:14], refs[14]
    copies = [pltpu.make_async_copy(a, b, sem.at[i]) for i, (a, b) in enumerate(zip(sources, targets))]
    for copy in copies:
        copy.start()
    for copy in copies:
        copy.wait()


def shards(prompt, gain_first, gate_first, up_first, down_first, gain_second, gate_second, up_second, down_second):
    plan = build_plan()
    rows, width = prompt.shape
    units = gate_first.shape[1]
    depth, columns = down_first.shape
    count = len(plan.copies)
    sem, vmem = pltpu.SemaphoreType.DMA, pltpu.VMEM
    block = rows // 8
    tall = jax.ShapeDtypeStruct((units, width), BF16)
    shapes = (tall,) * 6 + (jax.ShapeDtypeStruct((block, width), BF16),)
    outs = pl.pallas_call(
        functools.partial(kernel, plan),
        out_shape=shapes,
        in_specs=[pl.BlockSpec(memory_space=pltpu.HBM)] * 9,
        out_specs=(pl.BlockSpec(memory_space=vmem),) * 7,
        scratch_shapes=[
            vmem((rows, width), BF16),
            vmem((rows, width), BF16),
            vmem((rows, units), BF16),
            vmem((2, rows, width), BF16),
            vmem((block, width), F32),
            *[vmem((width, units), BF16)] * 4,
            *[vmem((NX, 8, depth, columns), BF16)] * 2,
            vmem((2, depth, columns), BF16),
            *[vmem((NY, block, width), BF16)] * 2,
            *[vmem((2, block // 2, width), BF16)] * 2,
            *[vmem((2, block, width), BF16)] * 2,
            vmem((2, NY, block, width), BF16),
            vmem((2, 1, gain_first.shape[0]), F32),
            vmem((4, *gate_first.shape), F32),
            vmem((2, depth, columns), F32),
            sem((9,)),
            sem((count,)),
            sem((count,)),
            sem((2, 8)),
        ],
        compiler_params=pltpu.CompilerParams(collective_id=0, has_side_effects=True, vmem_limit_bytes=LIMIT),
        name="handover",
    )(
        *[
            pltpu.with_memory_space_constraint(a, pltpu.HBM)
            for a in (
                prompt,
                gain_first.reshape(1, -1), gate_first, up_first, down_first,
                gain_second.reshape(1, -1), gate_second, up_second, down_second,
            )
        ],
    )
    outs = pl.pallas_call(
        hand_out,
        out_shape=shapes,
        in_specs=[pl.BlockSpec(memory_space=vmem)] * 7,
        out_specs=(pl.BlockSpec(memory_space=pl.ANY),) * 7,
        scratch_shapes=[sem((7,))],
        compiler_params=pltpu.CompilerParams(vmem_limit_bytes=16 * 1024 * 1024),
        name="hand_out",
    )(*outs)
    return (outs[0].T, outs[1].T, outs[2], outs[3].T, outs[4].T, outs[5], outs[6])


LIMIT = 44 * 1024 * 1024


def solution(mesh):
    rows = P(("gr", "fs"), None)
    block = P(("gr", "fs"), "tp")
    line = P(("gr", "fs"))
    return jax.shard_map(
        shards,
        mesh=mesh,
        in_specs=(rows, line, block, block, block, line, block, block, block),
        out_specs=(
            P(None, "tp"),
            P(None, "tp"),
            P("tp", None),
            P(None, "tp"),
            P(None, "tp"),
            P("tp", None),
            P(("gr", "fs", "tp"), None),
        ),
        check_vma=False,
    )
```

```python
import functools
import heapq

import jax
import jax.numpy as jnp
from jax import lax
from jax.experimental import pallas as pl
from jax.experimental.pallas import tpu as pltpu
from jax.sharding import PartitionSpec as P

MESH = pl.DeviceIdType.MESH
F32, BF16 = jnp.float32, jnp.bfloat16
NX, NY, NZ = 4, 4, 8
CHUNKS = 4
WAVES = 2
WAVE = 64 // WAVES
GROUPS = ((2,), (1, 3), (0,))

UNIT, SQUARE, DOWN, ROWS, PAIR, WIRE, NEAR = 1.08, 1.0, 2.15, 5.7, 0.5, 2.0, 1.0

ZP, ZM, XP, XM, YP, YM, PR = LINKS = range(7)
STEP = {ZP: (1, 0, 0), ZM: (-1, 0, 0), XP: (0, 1, 0), XM: (0, -1, 0), YP: (0, 0, 1), YM: (0, 0, -1), PR: (0, 0, 0)}
G, U, D, N, R, E = range(6)
BEGIN, START, NORM, HIDE, GLUE, TURN, PART, SUM, LAST, SOURCE, PASS = range(100, 111)
OWN, ALONG, ACROSS, PAIRED, FAR, CLOSE, GIVE = range(200, 207)


class Copy:
    def __init__(self, idx, link, dur, at):
        self.idx, self.link, self.dur = idx, link, dur
        self.buf = at["buf"]
        self.at = at
        self.rank = 0


class Task:
    def __init__(self, needs, dur, sends, rank, only):
        self.needs, self.dur, self.sends, self.rank, self.only = list(needs), dur, list(sends), rank, only

    def falls_to(self, d):
        return self.only is None or min(d, NZ - d) == self.only


class Plan:
    def __init__(self):
        self.copies, self.tasks = {}, {}

    def copy(self, key, link, dur, **at):
        self.copies[key] = Copy(len(self.copies), link, dur, at)
        return key

    def task(self, key, needs, dur, sends=(), rank=0, only=None):
        self.tasks[key] = Task(needs, dur, sends, rank, only)

    def starts_here(self, c, d):
        if c.buf != D or c.at["kind"] == ACROSS:
            return True
        if c.at["kind"] == OWN:
            return d != 0
        return d < 4 if c.link == ZP else d == 0 or d > 5

    def absent(self, need, d):
        if need in self.tasks:
            return not self.tasks[need].falls_to(d)
        copy = self.copies.get(need)
        if copy is None or copy.buf != D:
            return False
        if copy.at["kind"] == OWN:
            return d != 0
        return copy.at["kind"] == ALONG and (d == 0 or (copy.link == ZP) != (d < 5))

    def simulate(self, fixed=None):
        kinds = [(d, c) for d in range(NZ) for c in range(2)]
        left = {k: {t: {n for n in v.needs if not self.absent(n, k[0])} for t, v in self.tasks.items() if v.falls_to(k[0])} for k in kinds}
        users = {}
        for t, v in self.tasks.items():
            for n in v.needs:
                users.setdefault(n, []).append(t)
        place = {t: i for i, t in enumerate(self.tasks)}
        ready, pending, turn = {k: [] for k in kinds}, {}, {k: 0 for k in kinds}
        free, busy = {}, {k: 0.0 for k in kinds}
        starts = {k: {} for k in kinds}
        events, self.count = [], 0

        def at_time(at, k, link, what):
            self.count += 1
            heapq.heappush(events, (at, self.count, k, link, what))

        def enable(k, t, at):
            rank = self.tasks[t].rank
            heapq.heappush(ready[k], (rank, place[t] if rank else at, place[t], t))

        def start(k, key, only, now):
            copy = self.copies[key]
            d, c = k
            starts[k][key, only] = now
            end = free[k, copy.link] = max(now, free.get((k, copy.link), 0.0)) + copy.dur
            dz, _, dy = STEP[copy.link]
            to = ((d + dz - 2 * dy) % NZ, c)
            if copy.buf == D and copy.at["kind"] == OWN:
                to = (0, c)
            if copy.link == PR:
                to = ((d + (-1 if c == 0 else 1)) % NZ, 1 - c)
            at_time(end + (NEAR if copy.link == PR else WIRE), to, None, key)

        for k in kinds:
            for t in left[k]:
                if not left[k][t]:
                    enable(k, t, 0.0)
            at_time(0.0, k, None, None)
        while events:
            now, _, k, link, what = heapq.heappop(events)
            if link is not None:
                queue = pending[k, link]
                if queue and now >= free.get((k, link), 0.0) - AHEAD - 1e-9:
                    _, _, key, only = heapq.heappop(queue)
                    start(k, key, only, now)
                if queue:
                    at_time(max(now, free[k, link] - AHEAD), k, link, None)
                continue
            for t in users.get(what, ()) if what is not None else ():
                if what in left[k].get(t, ()):
                    left[k][t].discard(what)
                    if not left[k][t]:
                        enable(k, t, now)
            if what in self.tasks and fixed is None:
                task = self.tasks[what]
                for key in task.sends:
                    copy = self.copies[key]
                    if self.starts_here(copy, k[0]):
                        self.count += 1
                        heapq.heappush(pending.setdefault((k, copy.link), []), (copy.rank, self.count, key, task.only))
                        at_time(max(now, free.get((k, copy.link), 0.0) - AHEAD), k, copy.link, None)
            if now < busy[k]:
                continue
            if fixed is None:
                if not ready[k]:
                    continue
                t = heapq.heappop(ready[k])[3]
            else:
                t = None
                while turn[k] < len(fixed):
                    key, only = fixed[turn[k]]
                    if key in self.tasks:
                        if key in left[k]:
                            if not left[k][key]:
                                t = key
                                turn[k] += 1
                            break
                    elif (only is None or min(k[0], NZ - k[0]) == only) and self.starts_here(self.copies[key], k[0]):
                        start(k, key, only, now)
                    turn[k] += 1
                if t is None:
                    continue
            starts[k][t, None] = now
            busy[k] = now + self.tasks[t].dur
            at_time(busy[k], k, None, t)
        if fixed is not None and any(turn[k] < len(fixed) for k in kinds):
            return starts, 1e9
        return starts, max(busy.values())

    def find_before(self):
        starters, self.before = {}, {}
        for t, v in self.tasks.items():
            for c in v.sends:
                starters.setdefault(c, []).append((c, v.only))
                self.before[c, v.only] = [(t, None)]
        for t, v in self.tasks.items():
            before = [(n, None) for n in v.needs if n in self.tasks]
            for n in v.needs:
                for c, m in starters.get(n, ()):
                    hop = self.copies[n].buf == D and self.copies[n].at["kind"] == ALONG
                    if m is None or v.only is None or m == v.only - hop:
                        before.append((c, m))
            self.before[t, None] = before

    def line_up(self, starts, mix):
        at = {}
        for e in self.before:
            here = [v[e] for v in starts.values() if e in v]
            at[e] = mix * max(here) + (1 - mix) * sum(here) / len(here) if here else 0.0
        place = {e: i for i, e in enumerate(self.before)}
        changed = True
        while changed:
            changed = False
            for e, before in self.before.items():
                for n in before:
                    if at[n] >= at[e]:
                        at[e] = at[n] + 1e-6
                        changed = True
        return sorted(self.before, key=lambda e: (at[e], place[e]))

    def order(self):
        self.find_before()
        starts, self.ideal = self.simulate()
        best = None
        for mix in (0.0, 0.2, 0.4, 0.6, 0.8, 1.0):
            line = self.line_up(starts, mix)
            total = self.simulate(line)[1]
            if best is None or total < best[0]:
                best = total, line
        self.total = best[0]
        return best[1]


GATE = (PASS, G, 1, ALONG, 0, 2)
AHEAD = 2.0
RANKS = [3, 0, -2, 8, 1, 10, 2, 0, 5, 10, 1, 36, 60, -24]


def rank_copies(p):
    for key, c in p.copies.items():
        if c.buf not in (G, U, D, E):
            continue
        l = c.at["layer"]
        if c.link in (YP, YM):
            r = 0
        elif c.link in (ZP, ZM):
            if c.buf == D:
                r = RANKS[0]
            elif c.buf in (G, E):
                r = RANKS[1] + RANKS[2] * key[-1]
            else:
                r = RANKS[3] + RANKS[4] * key[-1]
        elif c.buf == U:
            r = RANKS[5] if len(key) == 4 else RANKS[6]
        elif c.buf in (G, E):
            far = c.at["x"] == 2
            r = RANKS[9] if far else RANKS[7] if key[2] == OWN else RANKS[8]
        else:
            r = RANKS[11] if c.at["x"] == 2 else RANKS[10]
        c.rank = r + RANKS[12] * l + RANKS[13] * (c.buf == E)


def build_plan():
    p = Plan()
    whole, downs, blocks = ([], []), ([], []), {}
    signs = ((0, -1), (1, 1))
    zs, xs = (ZP, ZM), (XP, XM)

    p.task((BEGIN,), [], 3.0, [p.copy((D, 1, OWN), YP, 2.0, buf=D, layer=1, kind=OWN)])
    for l in (0, 1):

        def put(buf, link, zrel, xrel, half, *tag):
            key = (buf, l, *tag)
            unit = SQUARE if buf == E else UNIT
            p.copy(key, link, unit * (1.0 if half is None else 0.5), buf=buf, layer=l, z=zrel, x=xrel, half=half)
            (blocks.setdefault(zrel % NZ, []) if buf == E else whole[l]).append(key)
            return key

        z_first = (G, E) if l == 0 else (G,)
        first = []
        for s, sign in signs:
            first += [put(b, zs[s], sign, 0, None, ALONG, s, 1) for b in z_first]
            first += [put(U, xs[s], 0, sign, None, ACROSS, s)]
            first += [put(U, zs[s], sign, 0, None, ALONG, 0, s, 1)]
            first += [put(b, xs[s], 0, sign, None, OWN, s) for b in z_first]
        p.task((START, l), [(BEGIN,)] if l == 0 else [(START, 0)], 0.2, first)

        for b in z_first:
            for s, sign in signs:
                p.task((PASS, b, l, OWN, s), [(b, l, OWN, s)], 0.03, [put(b, xs[s], 0, 2, s, OWN, s, 2)])
                for step in (1, 2, 3, 4):
                    zrel, half = sign * step, s if step == 4 else None
                    sends = []
                    if step < 4:
                        sends.append(put(b, zs[s], sign * (step + 1), 0, s if step == 3 else None, ALONG, s, step + 1))
                    for t, to in signs:
                        sends.append(put(b, xs[t], zrel, to, half, ACROSS, s, step, t))
                    p.task((PASS, b, l, ALONG, s, step), [(b, l, ALONG, s, step)], 0.03, sends)
                    far = put(b, xs[s], zrel, 2, half, ACROSS, s, step, 2)
                    p.task((PASS, b, l, ACROSS, s, step), [(b, l, ACROSS, s, step, s)], 0.03, [far])
        for s, sign in signs:
            p.task((PASS, U, l, ACROSS, s), [(U, l, ACROSS, s)], 0.03, [put(U, xs[s], 0, 2, s, ACROSS, s, 2)])
            sends = [put(U, zs[t], to, sign, None, ALONG, 1 + s, t, 1) for t, to in signs]
            p.task((PASS, U, l, ALONG, 1 + s), [(U, l, ACROSS, s)], 0.03, sends)
        sends = [put(U, zs[t], to, 2, None, ALONG, 3, t, 1) for t, to in signs]
        p.task((PASS, U, l, ALONG, 3), [(U, l, ACROSS, 0, 2), (U, l, ACROSS, 1, 2)], 0.03, sends)
        for column, xrel in enumerate((0, -1, 1, 2)):
            for t, sign in signs:
                for step in range(1, 4 if (t == 0) == (column in (0, 2)) else 3):
                    c = put(U, zs[t], sign * (step + 1), xrel, None, ALONG, column, t, step + 1)
                    p.task((PASS, U, l, ALONG, column, t, step), [(U, l, ALONG, column, t, step)], 0.03, [c])

    for k in range(NZ):
        c = p.copy((E, 0, GIVE, k), (YP, YM)[k % 2], 3.9, buf=E, layer=0, k=k)
        p.task((PASS, E, 0, GIVE, k), blocks[k], 0.05, [c])
        downs[0].extend([c, (PASS, E, 0, GIVE, k)])
    l, along = 1, {}
    for k in range(CHUNKS):
        for s, sign in signs:
            along[k, s] = p.copy((D, l, ALONG, k, s), zs[s], DOWN, buf=D, layer=l, kind=ALONG, chunk=k)
        sends = [along[k, 0], along[k, 1]]
        sends += [p.copy((D, l, ACROSS, k, s), xs[s], DOWN, buf=D, layer=l, kind=ACROSS, chunk=k, x=sign) for s, sign in signs]
        s = k % 2
        c = p.copy((D, l, ACROSS, k, 2), xs[s], DOWN, buf=D, layer=l, kind=ACROSS, chunk=k, x=2)
        for m in range(NZ // 2 + 1):
            needs = [(SOURCE, l)] if m == 0 else [along[k, 0], along[k, 1]]
            p.task((PASS, D, l, ALONG, k, m), needs, 0.05, sends, only=m)
            p.task((PASS, D, l, ACROSS, k, m), [(D, l, ACROSS, k, s)], 0.03, [c], only=m)
            downs[l].append((PASS, D, l, ALONG, k, m))
        downs[l].extend([sends[2], sends[3], c])
    p.task((SOURCE, l), [(D, l, OWN), GATE], 0.1, [], only=0)

    p.task((NORM,), [(START, 0)], 2.0, rank=1)
    p.task((HIDE, 0), [(NORM,)] + whole[0], 3.0, rank=1)
    p.task((GLUE, 0), downs[0], 0.8, rank=1)
    add_reduce(p, 0, [(HIDE, 0), (GLUE, 0)])
    for w in range(WAVES):
        for s, sign in signs:
            c = p.copy((N, w, CLOSE, s), (YP, YM)[s], ROWS / WAVES, buf=N, wave=w, y=sign, half=None, core=0)
            p.tasks[LAST, 0, w].sends.append(c)
            far = p.copy((N, w, FAR, s), (YP, YM)[s], ROWS / WAVES / 2, buf=N, wave=w, y=2, half=s, core=0)
            near = p.copy((N, w, PAIRED, s), PR, PAIR / WAVES, buf=N, wave=w, y=sign, half=None, core=1)
            p.task((PASS, N, w, CLOSE, s), [c], 0.03, [far, near])
            c = p.copy((N, w, PAIRED, FAR, s), PR, PAIR / WAVES / 2, buf=N, wave=w, y=2, half=s, core=1)
            p.task((PASS, N, w, FAR, s), [far], 0.03, [c])
        p.tasks[LAST, 0, w].sends.append(p.copy((N, w, PAIRED), PR, PAIR / WAVES, buf=N, wave=w, y=0, half=None, core=1))
        rows = {
            (0,): [(LAST, 0, w), (N, w, PAIRED)],
            (1, 3): [(N, w, CLOSE, 0), (N, w, PAIRED, 0), (N, w, CLOSE, 1), (N, w, PAIRED, 1)],
            (2,): [(N, w, FAR, 0), (N, w, FAR, 1), (N, w, PAIRED, FAR, 0), (N, w, PAIRED, FAR, 1)],
        }
        for rs in GROUPS[::-1]:
            p.task((HIDE, 1, w, rs), rows[rs] + whole[1], 1.2, rank=1)
    p.task((GLUE, 1), downs[1], 0.8, rank=1)
    add_reduce(p, 1, [(GLUE, 1)])
    for l in (0, 1):
        for buf in (G, U):
            for part in (0, 1):
                p.task((TURN, buf, l, part), whole[l] + [(HIDE, 0)], 0.5, rank=2)
    rank_copies(p)
    p.sequence = p.order()
    return p


def add_reduce(p, l, needs):
    for w in range(WAVES):
        for rs in GROUPS:
            c = [p.copy((R, l, w, PAIRED, r), PR, PAIR / WAVES, buf=R, layer=l, wave=w, kind=PAIRED, rel=r) for r in rs]
            p.task((PART, l, w, rs), needs + ([(HIDE, 1, w, rs)] if l else []), 0.7, c, rank=1)
        far, near = [
            [p.copy((R, l, w, kind, s), (YP, YM)[s], ROWS / WAVES / part, buf=R, layer=l, wave=w, kind=kind, side=s) for s in (0, 1)]
            for kind, part in ((FAR, 2), (CLOSE, 1))
        ]
        p.task((SUM, l, w, 2), [(PART, l, w, (2,)), (R, l, w, PAIRED, 2)], 0.15, far)
        for s, r in enumerate((1, 3)):
            p.task((SUM, l, w, r), [(PART, l, w, (1, 3)), (R, l, w, PAIRED, r), far[s]], 0.15, [near[s]])
        p.task((LAST, l, w), [(PART, l, w, (0,)), (R, l, w, PAIRED, 0)] + near, 0.4)


def normalized(rows):
    scale = lax.rsqrt(jnp.mean(rows * rows, axis=-1, keepdims=True) + 1e-06)
    return (rows * scale).astype(BF16)


def gated(normed, w_gate, w_up):
    gate = jnp.dot(normed, w_gate, preferred_element_type=F32)
    upper = jnp.dot(normed, w_up, preferred_element_type=F32)
    return (gate / (1.0 + jnp.exp(-gate)) * upper).astype(BF16)


def kernel(
    plan,
    prompt_hbm,
    gain_a, gate_a, up_a, down_a,
    gain_b, gate_b, up_b, down_b,
    gt0, ut0, t0, gt1, ut1, t1, mixed,
    prompt, normed, hidden, part, stream,
    g0, u0, g1, u1, squares, given, d1, stage,
    pair0, pair1, far0, far1, near0, near1, sums,
    gains, gates, depths,
    load_sem, send_sem, recv_sem, own_sem,
):
    gr, fs, tp = lax.axis_index("gr"), lax.axis_index("fs"), lax.axis_index("tp")
    z = gr * 4 + fs // 4
    x = lax.rem(fs, 4)
    y = tp // 2
    core = lax.rem(tp, 2)

    def device(xx, yy, zz, cc):
        return (zz // 4, lax.rem(zz, 4) * 4 + xx, yy * 2 + cc)

    def zat(k):
        return lax.rem(z + (k % NZ), NZ) if k % NZ else z

    def xat(k):
        return lax.rem(x + (k % NX), NX) if k % NX else x

    def yat(k):
        return lax.rem(y + (k % NY), NY) if k % NY else y

    other = 1 - core
    peers = {
        ZP: device(x, y, zat(1), core),
        ZM: device(x, y, zat(-1), core),
        XP: device(xat(1), y, z, core),
        XM: device(xat(-1), y, z, core),
        YP: device(x, yat(1), z, core),
        YM: device(x, yat(-1), z, core),
        PR: device(x, y, z, other),
    }
    weights = {(G, 0): g0, (U, 0): u0, (G, 1): g1, (U, 1): u1}
    turned = {(G, 0): gt0, (U, 0): ut0, (G, 1): gt1, (U, 1): ut1}
    talls = (t0, t1)
    pairs, fars, nears = (pair0, pair1), (far0, far1), (near0, near1)
    dist = lax.rem(z + NZ - tp, NZ)

    def rows_at(ref, row, half):
        if half is None:
            return ref.at[pl.ds(pl.multiple_of(row, 64), 64), :]
        return ref.at[pl.ds(pl.multiple_of(row + 32 * half, 32), 32), :]

    def refs(c, sender):
        dz, dx, dy = STEP[c.link] if sender else (0, 0, 0)
        at = c.at
        if c.buf == E:
            if "k" in at:
                return squares.at[pl.ds(zat(at["k"]) * NX, NX)], given.at[tp]
            ref = squares.at[zat(at["z"] + dz) * NX + xat(at["x"] + dx)]
            if at["half"] is not None:
                ref = ref.at[:, pl.ds(128 * at["half"], 128)]
            return ref, ref
        if c.buf in (G, U):
            row = (zat(at["z"] + dz) * NX + xat(at["x"] + dx)) * 64
            ref = rows_at(weights[c.buf, at["layer"]], row, at["half"])
            return ref, ref
        if c.buf == D:
            n = 8 // CHUNKS
            ref = d1.at[xat(at.get("x", 0) + dx), pl.ds(at["chunk"] * n, n)]
            return ref, ref
        w = at["wave"]
        if c.buf == N:
            cc = other if at["core"] and not sender else core
            row, size = (yat(at["y"] + dy) * 2 + cc) * 64 + WAVE * w, WAVE
            if at["half"] is not None:
                row, size = row + WAVE // 2 * at["half"], WAVE // 2
            ref = normed.at[pl.ds(pl.multiple_of(row, WAVE // 2), size), :]
            return ref, ref
        l, wave = at["layer"], pl.ds(WAVE * w, WAVE)
        if at["kind"] == PAIRED:
            row = (yat(at["rel"]) * 2 + other) * 64 + WAVE * w
            return part.at[l, pl.ds(pl.multiple_of(row, WAVE), WAVE), :], pairs[l].at[at["rel"], wave, :]
        side = at["side"]
        if at["kind"] == FAR:
            half = WAVE // 2
            return sums.at[l, 2, pl.ds(WAVE * w + half * side, half), :], fars[l].at[side, pl.ds(half * w, half), :]
        return sums.at[l, 1 + 2 * side, wave, :], nears[l].at[side, wave, :]

    def describe(c, sender):
        src, dst = refs(c, sender)
        return pltpu.make_async_remote_copy(
            src_ref=src,
            dst_ref=dst,
            send_sem=send_sem.at[c.idx],
            recv_sem=recv_sem.at[c.idx],
            device_id=peers[c.link],
            device_id_type=MESH,
        )

    def own_copy(c, t):
        return pltpu.make_async_remote_copy(
            src_ref=stage,
            dst_ref=d1.at[x, t],
            send_sem=send_sem.at[c.idx],
            recv_sem=own_sem.at[1, t],
            device_id=device(x, z // 2, z, lax.rem(z, 2)),
            device_id_type=MESH,
        )

    def given_copy(c, t):
        src, _ = refs(c, True)
        to = zat(c.at["k"])
        return pltpu.make_async_remote_copy(
            src_ref=src,
            dst_ref=given.at[t],
            send_sem=send_sem.at[c.idx],
            recv_sem=own_sem.at[0, t],
            device_id=(gr, fs, to),
            device_id_type=MESH,
        )

    def passes(c):
        if "k" in c.at:
            return zat(c.at["k"]) != tp
        if c.buf != D or c.at["kind"] == ACROSS:
            return None
        if c.at["kind"] == OWN:
            return dist != 0
        return dist < 4 if c.link == ZP else jnp.logical_or(dist == 0, dist > 5)

    def if_so(here, act):
        if here is None:
            act()
        else:
            pl.when(here)(act)

    def is_own(c):
        return c.buf == D and c.at["kind"] == OWN

    def outgoing(c):
        return given_copy(c, tp) if "k" in c.at else own_copy(c, tp) if is_own(c) else describe(c, True)

    def send(c, here):
        if_so(here, outgoing(c).start)

    def sent(c):
        if_so(passes(c), outgoing(c).wait_send)

    seen = set()

    def arrived(key, only):
        c = plan.copies[key]
        if "k" in c.at:
            t = c.at["k"]
            if_so(tp != t, given_copy(c, t).wait_recv)
            return
        if c.buf == D and c.at["kind"] == ALONG:
            if_so(dist == (only if c.link == ZP else NZ - only), describe(c, False).wait_recv)
            return
        if (key, only) in seen or (only is None and (key, 4) in seen):
            return
        seen.add((key, only))
        if is_own(c):
            for t in range(8):
                if_so(jnp.logical_and(dist == 0, tp != t), own_copy(c, t).wait_recv)
            return
        here = None if only is None else hops == only
        if_so(here, describe(c, False).wait_recv)

    hops = jnp.minimum(dist, NZ - dist)
    eye = lax.broadcasted_iota(jnp.int32, (64, 64), 0) == lax.broadcasted_iota(jnp.int32, (64, 64), 1)

    def fold(gain, w):
        column = jnp.sum(jnp.where(eye, gain[...], 0.0), axis=1, keepdims=True)
        return (column * w[...]).astype(BF16)

    mine = pl.ds(pl.multiple_of((z * NX + x) * 64, 64), 64)

    def rows_of(r, cc, w):
        return pl.ds(pl.multiple_of((yat(r) * 2 + cc) * 64 + WAVE * w, WAVE), WAVE)

    def group(rs, w):
        return [rows_of(r, cc, w) for r in rs for cc in (0, 1)]

    loads = [
        pltpu.make_async_copy(src, dst, load_sem.at[i])
        for i, (src, dst) in enumerate(
            (
                (gain_a, gains.at[0]), (gate_a, gates.at[0]), (up_a, gates.at[1]), (down_a, depths.at[0]),
                (gain_b, gains.at[1]), (gate_b, gates.at[2]), (up_b, gates.at[3]), (down_b, depths.at[1]),
                (prompt_hbm, prompt),
            )
        )
    ]

    def begin():
        for load in loads:
            load.start()
        barrier = pltpu.get_barrier_semaphore()
        greet = [peers[k] for k in (ZP, ZM, XP, XM)]
        greet += [(gr, fs, lax.rem(tp + k, 8)) for k in range(1, 8)]
        for who in greet:
            pl.semaphore_signal(barrier, inc=1, device_id=who, device_id_type=MESH)
        for load in loads[:8]:
            load.wait()
        for i, ref in enumerate((g0, u0, g1, u1)):
            ref[mine, :] = fold(gains.at[i // 2], gates.at[i])
        squares[z * NX + x] = depths[0].astype(BF16)
        stage[...] = depths[1].astype(BF16)

        @pl.when(dist == 0)
        def _():
            d1[x, tp] = depths[1].astype(BF16)

        pl.semaphore_wait(barrier, len(greet))

    def norm():
        loads[8].wait()

        @pl.loop(0, 8)
        def _(i):
            at = pl.ds(pl.multiple_of(i * 64, 64), 64)
            normed[at, :] = normalized(prompt[at, :].astype(F32))

    def hide(l, w=None, rs=None):
        if l == 0:

            @pl.loop(0, 2)
            def _(i):
                at = pl.ds(pl.multiple_of(i * 256, 256), 256)
                hidden[at, :] = gated(normed[at, :], g0[...], u0[...])

            return
        spots = group(rs, w)
        out = gated(jnp.concatenate([normed[at, :] for at in spots], axis=0), g1[...], u1[...])
        for i, at in enumerate(spots):
            hidden[at, :] = out[WAVE * i : WAVE * (i + 1)]

    def turn(buf, l, piece):
        src, dst = weights[buf, l], turned[buf, l]

        @pl.loop(0, 4)
        def _(i):
            at = pl.ds(pl.multiple_of((piece * 4 + i) * 256, 256), 256)
            dst[:, at] = src[at, :].astype(F32).T.astype(BF16)

    def glue(l):
        if l == 0:
            for k in range(NX):
                given[tp, k] = squares[tp * NX + k]
        for t in range(8):
            blocks = [(given[t, k] if l == 0 else d1[k, t]).astype(F32) for k in range(NX)]
            rows = jnp.concatenate(blocks, axis=0)
            talls[l][:, 256 * t : 256 * (t + 1)] = rows.astype(BF16)

    def partial(l, w, rs):
        spots = group(rs, w)
        rows = jnp.concatenate([hidden[at, :] for at in spots], axis=0)
        out = jnp.dot(rows, talls[l][...], preferred_element_type=F32).astype(BF16)
        for i, at in enumerate(spots):
            part[l, at, :] = out[WAVE * i : WAVE * (i + 1)]

    def chip_sum(l, w, r):
        wave = slice(WAVE * w, WAVE * (w + 1))
        return part[l, rows_of(r, core, w), :].astype(F32) + pairs[l][r, wave, :].astype(F32)

    def add_up(l, w, r):
        total, half = chip_sum(l, w, r), WAVE // 2
        lower, upper = slice(WAVE * w, WAVE * w + half), slice(WAVE * w + half, WAVE * (w + 1))
        first, second = total[:half], total[half:]
        if r == 1:
            first = first + fars[l][0, half * w : half * (w + 1), :].astype(F32)
        if r == 3:
            second = second + fars[l][1, half * w : half * (w + 1), :].astype(F32)
        sums[l, r, lower, :] = first.astype(BF16)
        sums[l, r, upper, :] = second.astype(BF16)

    def last(l, w):
        wave = slice(WAVE * w, WAVE * (w + 1))
        total = chip_sum(l, w, 0) + nears[l][0, wave, :].astype(F32) + nears[l][1, wave, :].astype(F32)
        if l == 0:
            at = rows_of(0, core, w)
            rows = prompt[at, :].astype(F32) + 0.5 * total
            stream[wave, :] = rows
            normed[at, :] = normalized(rows)
        else:
            mixed[wave, :] = (stream[wave, :] + 0.5 * total).astype(BF16)

    work = {BEGIN: begin, NORM: norm, HIDE: hide, TURN: turn, GLUE: glue, PART: partial, SUM: add_up, LAST: last}
    for key, only in plan.sequence:
        if key in plan.copies:
            c = plan.copies[key]
            here = passes(c)
            if only is not None:
                here = hops == only if here is None else jnp.logical_and(here, hops == only)
            send(c, here)
            continue
        task = plan.tasks[key]
        for n in task.needs:
            if n in plan.copies and not (task.only == 4 and plan.copies[n].link == ZM and plan.copies[n].at.get("kind") == ALONG):
                arrived(n, task.only)
        if key[0] in work:
            work[key[0]](*key[1:])
    for c in plan.copies.values():
        sent(c)


def hand_out(*refs):
    sources, targets, sem = refs[:7], refs[7:14], refs[14]
    copies = [pltpu.make_async_copy(a, b, sem.at[i]) for i, (a, b) in enumerate(zip(sources, targets))]
    for copy in copies:
        copy.start()
    for copy in copies:
        copy.wait()


def shards(prompt, gain_first, gate_first, up_first, down_first, gain_second, gate_second, up_second, down_second):
    plan = build_plan()
    rows, width = prompt.shape
    units = gate_first.shape[1]
    depth, columns = down_first.shape
    count = len(plan.copies)
    sem, vmem = pltpu.SemaphoreType.DMA, pltpu.VMEM
    block = rows // 8
    tall = jax.ShapeDtypeStruct((units, width), BF16)
    shapes = (tall,) * 6 + (jax.ShapeDtypeStruct((block, width), BF16),)
    outs = pl.pallas_call(
        functools.partial(kernel, plan),
        out_shape=shapes,
        in_specs=[pl.BlockSpec(memory_space=pltpu.HBM)] * 9,
        out_specs=(pl.BlockSpec(memory_space=vmem),) * 7,
        scratch_shapes=[
            vmem((rows, width), BF16),
            vmem((rows, width), BF16),
            vmem((rows, units), BF16),
            vmem((2, rows, width), BF16),
            vmem((block, width), F32),
            *[vmem((width, units), BF16)] * 4,
            vmem((NX * NZ, depth, columns), BF16),
            vmem((8, NX, depth, columns), BF16),
            vmem((NX, 8, depth, columns), BF16),
            vmem((depth, columns), BF16),
            *[vmem((NY, block, width), BF16)] * 2,
            *[vmem((2, block // 2, width), BF16)] * 2,
            *[vmem((2, block, width), BF16)] * 2,
            vmem((2, NY, block, width), BF16),
            vmem((2, 1, gain_first.shape[0]), F32),
            vmem((4, *gate_first.shape), F32),
            vmem((2, depth, columns), F32),
            sem((9,)),
            sem((count,)),
            sem((count,)),
            sem((2, 8)),
        ],
        compiler_params=pltpu.CompilerParams(collective_id=0, has_side_effects=True, vmem_limit_bytes=LIMIT),
        name="handover",
    )(
        *[
            pltpu.with_memory_space_constraint(a, pltpu.HBM)
            for a in (
                prompt,
                gain_first.reshape(1, -1), gate_first, up_first, down_first,
                gain_second.reshape(1, -1), gate_second, up_second, down_second,
            )
        ],
    )
    outs = pl.pallas_call(
        hand_out,
        out_shape=shapes,
        in_specs=[pl.BlockSpec(memory_space=vmem)] * 7,
        out_specs=(pl.BlockSpec(memory_space=pl.ANY),) * 7,
        scratch_shapes=[sem((7,))],
        compiler_params=pltpu.CompilerParams(vmem_limit_bytes=16 * 1024 * 1024),
        name="hand_out",
    )(*outs)
    return (outs[0].T, outs[1].T, outs[2], outs[3].T, outs[4].T, outs[5], outs[6])


LIMIT = 44 * 1024 * 1024


def solution(mesh):
    rows = P(("gr", "fs"), None)
    block = P(("gr", "fs"), "tp")
    line = P(("gr", "fs"))
    return jax.shard_map(
        shards,
        mesh=mesh,
        in_specs=(rows, line, block, block, block, line, block, block, block),
        out_specs=(
            P(None, "tp"),
            P(None, "tp"),
            P("tp", None),
            P(None, "tp"),
            P(None, "tp"),
            P("tp", None),
            P(("gr", "fs", "tp"), None),
        ),
        check_vma=False,
    )
```

```python
import functools
import heapq

import jax
import jax.numpy as jnp
from jax import lax
from jax.experimental import pallas as pl
from jax.experimental.pallas import tpu as pltpu
from jax.sharding import PartitionSpec as P

MESH = pl.DeviceIdType.MESH
F32, BF16 = jnp.float32, jnp.bfloat16
NX, NY, NZ = 4, 4, 8
CHUNKS = 4
WAVES = 2
WAVE = 64 // WAVES
GROUPS = ((2,), (1, 3), (0,))

UNIT, SQUARE, DOWN, ROWS, PAIR, WIRE, NEAR = 1.15, 1.05, 2.1, 5.7, 0.5, 2.1, 1.0

ZP, ZM, XP, XM, YP, YM, PR = LINKS = range(7)
STEP = {ZP: (1, 0, 0), ZM: (-1, 0, 0), XP: (0, 1, 0), XM: (0, -1, 0), YP: (0, 0, 1), YM: (0, 0, -1), PR: (0, 0, 0)}
G, U, D, N, R, E = range(6)
BEGIN, START, NORM, HIDE, GLUE, TURN, PART, SUM, LAST, SOURCE, PASS = range(100, 111)
OWN, ALONG, ACROSS, PAIRED, FAR, CLOSE, GIVE = range(200, 207)


class Copy:
    def __init__(self, idx, link, dur, at):
        self.idx, self.link, self.dur = idx, link, dur
        self.buf = at["buf"]
        self.at = at
        self.rank = 0


class Task:
    def __init__(self, needs, dur, sends, rank, only):
        self.needs, self.dur, self.sends, self.rank, self.only = list(needs), dur, list(sends), rank, only

    def falls_to(self, d):
        return self.only is None or min(d, NZ - d) == self.only


class Plan:
    def __init__(self):
        self.copies, self.tasks = {}, {}

    def copy(self, key, link, dur, **at):
        self.copies[key] = Copy(len(self.copies), link, dur, at)
        return key

    def task(self, key, needs, dur, sends=(), rank=0, only=None):
        self.tasks[key] = Task(needs, dur, sends, rank, only)

    def starts_here(self, c, d):
        if c.buf != D or c.at["kind"] == ACROSS:
            return True
        if c.at["kind"] == OWN:
            return d != 0
        return d < 4 if c.link == ZP else d == 0 or d > 5

    def absent(self, need, d):
        if need in self.tasks:
            return not self.tasks[need].falls_to(d)
        copy = self.copies.get(need)
        if copy is None or copy.buf != D:
            return False
        if copy.at["kind"] == OWN:
            return d != 0
        return copy.at["kind"] == ALONG and (d == 0 or (copy.link == ZP) != (d < 5))

    def simulate(self, fixed=None):
        kinds = [(d, c) for d in range(NZ) for c in range(2)]
        left = {k: {t: {n for n in v.needs if not self.absent(n, k[0])} for t, v in self.tasks.items() if v.falls_to(k[0])} for k in kinds}
        users = {}
        for t, v in self.tasks.items():
            for n in v.needs:
                users.setdefault(n, []).append(t)
        place = {t: i for i, t in enumerate(self.tasks)}
        ready, pending, turn = {k: [] for k in kinds}, {}, {k: 0 for k in kinds}
        free, busy = {}, {k: 0.0 for k in kinds}
        starts = {k: {} for k in kinds}
        events, self.count = [], 0

        def at_time(at, k, link, what):
            self.count += 1
            heapq.heappush(events, (at, self.count, k, link, what))

        def enable(k, t, at):
            rank = self.tasks[t].rank
            heapq.heappush(ready[k], (rank, place[t] if rank else at, place[t], t))

        def start(k, key, only, now):
            copy = self.copies[key]
            d, c = k
            starts[k][key, only] = now
            end = free[k, copy.link] = max(now, free.get((k, copy.link), 0.0)) + copy.dur
            dz, _, dy = STEP[copy.link]
            to = ((d + dz - 2 * dy) % NZ, c)
            if copy.buf == D and copy.at["kind"] == OWN:
                to = (0, c)
            if copy.link == PR:
                to = ((d + (-1 if c == 0 else 1)) % NZ, 1 - c)
            at_time(end + (NEAR if copy.link == PR else WIRE), to, None, key)

        for k in kinds:
            for t in left[k]:
                if not left[k][t]:
                    enable(k, t, 0.0)
            at_time(0.0, k, None, None)
        while events:
            now, _, k, link, what = heapq.heappop(events)
            if link is not None:
                queue = pending[k, link]
                if queue and now >= free.get((k, link), 0.0) - AHEAD - 1e-9:
                    _, _, key, only = heapq.heappop(queue)
                    start(k, key, only, now)
                if queue:
                    at_time(max(now, free[k, link] - AHEAD), k, link, None)
                continue
            for t in users.get(what, ()) if what is not None else ():
                if what in left[k].get(t, ()):
                    left[k][t].discard(what)
                    if not left[k][t]:
                        enable(k, t, now)
            if what in self.tasks and fixed is None:
                task = self.tasks[what]
                for key in task.sends:
                    copy = self.copies[key]
                    if self.starts_here(copy, k[0]):
                        self.count += 1
                        heapq.heappush(pending.setdefault((k, copy.link), []), (copy.rank, self.count, key, task.only))
                        at_time(max(now, free.get((k, copy.link), 0.0) - AHEAD), k, copy.link, None)
            if now < busy[k]:
                continue
            if fixed is None:
                if not ready[k]:
                    continue
                t = heapq.heappop(ready[k])[3]
            else:
                t = None
                while turn[k] < len(fixed):
                    key, only = fixed[turn[k]]
                    if key in self.tasks:
                        if key in left[k]:
                            if not left[k][key]:
                                t = key
                                turn[k] += 1
                            break
                    elif (only is None or min(k[0], NZ - k[0]) == only) and self.starts_here(self.copies[key], k[0]):
                        start(k, key, only, now)
                    turn[k] += 1
                if t is None:
                    continue
            starts[k][t, None] = now
            busy[k] = now + self.tasks[t].dur
            at_time(busy[k], k, None, t)
        if fixed is not None and any(turn[k] < len(fixed) for k in kinds):
            return starts, 1e9
        return starts, max(busy.values())

    def find_before(self):
        starters, self.before = {}, {}
        for t, v in self.tasks.items():
            for c in v.sends:
                starters.setdefault(c, []).append((c, v.only))
                self.before[c, v.only] = [(t, None)]
        for t, v in self.tasks.items():
            before = [(n, None) for n in v.needs if n in self.tasks]
            for n in v.needs:
                for c, m in starters.get(n, ()):
                    hop = self.copies[n].buf == D and self.copies[n].at["kind"] == ALONG
                    if m is None or v.only is None or m == v.only - hop:
                        before.append((c, m))
            self.before[t, None] = before

    def line_up(self, starts, mix):
        at = {}
        for e in self.before:
            here = [v[e] for v in starts.values() if e in v]
            at[e] = mix * max(here) + (1 - mix) * sum(here) / len(here) if here else 0.0
        place = {e: i for i, e in enumerate(self.before)}
        changed = True
        while changed:
            changed = False
            for e, before in self.before.items():
                for n in before:
                    if at[n] >= at[e]:
                        at[e] = at[n] + 1e-6
                        changed = True
        return sorted(self.before, key=lambda e: (at[e], place[e]))

    def order(self):
        self.find_before()
        starts, self.ideal = self.simulate()
        best = None
        for mix in (0.0, 0.2, 0.4, 0.6, 0.8, 1.0):
            line = self.line_up(starts, mix)
            total = self.simulate(line)[1]
            if best is None or total < best[0]:
                best = total, line
        self.total = best[0]
        return best[1]


GATE = (PASS, E, 0, ALONG, 0, 4)
RELAY = [(PASS, U, 0, ALONG, 2, 0, 3)] * 2
AHEAD = 2.0
RANKS = [1, 0, 3, 23, 1, 3, 18, 0, 29, 32, 10, 36, 30, -10]


def rank_copies(p):
    for key, c in p.copies.items():
        if c.buf not in (G, U, D, E):
            continue
        l = c.at["layer"]
        if c.link in (YP, YM):
            r = 0
        elif c.link in (ZP, ZM):
            if c.buf == D:
                r = RANKS[0]
            elif c.buf in (G, E):
                r = RANKS[1] + RANKS[2] * key[-1]
            else:
                r = RANKS[3] + RANKS[4] * key[-1]
        elif c.buf == U:
            r = RANKS[5] if len(key) == 4 else RANKS[6]
        elif c.buf in (G, E):
            far = c.at["x"] == 2
            r = RANKS[9] if far else RANKS[7] if key[2] == OWN else RANKS[8]
        else:
            r = RANKS[11] if c.at["x"] == 2 else RANKS[10]
        c.rank = r + RANKS[12] * l + RANKS[13] * (c.buf == E)


def build_plan():
    p = Plan()
    whole, downs, blocks = ([], []), ([], []), {}
    signs = ((0, -1), (1, 1))
    zs, xs = (ZP, ZM), (XP, XM)

    p.task((BEGIN,), [], 3.0, [p.copy((D, 1, OWN), YP, 2.0, buf=D, layer=1, kind=OWN)])
    for l in (0, 1):

        def put(buf, link, zrel, xrel, half, *tag):
            key = (buf, l, *tag)
            unit = SQUARE if buf == E else UNIT
            p.copy(key, link, unit * (1.0 if half is None else 0.5), buf=buf, layer=l, z=zrel, x=xrel, half=half)
            (blocks.setdefault(zrel % NZ, []) if buf == E else whole[l]).append(key)
            return key

        z_first = (G, E) if l == 0 else (G,)
        first = []
        for s, sign in signs:
            first += [put(b, zs[s], sign, 0, None, ALONG, s, 1) for b in z_first]
            first += [put(U, xs[s], 0, sign, None, ACROSS, s)]
            first += [put(U, zs[s], sign, 0, None, ALONG, 0, s, 1)]
            first += [put(b, xs[s], 0, sign, None, OWN, s) for b in z_first]
        p.task((START, l), [(BEGIN,)] if l == 0 else [(START, 0)], 0.2, first)

        for b in z_first:
            for s, sign in signs:
                p.task((PASS, b, l, OWN, s), [(b, l, OWN, s)], 0.03, [put(b, xs[s], 0, 2, s, OWN, s, 2)])
                for step in (1, 2, 3, 4):
                    zrel, half = sign * step, s if step == 4 else None
                    sends = []
                    if step < 4:
                        sends.append(put(b, zs[s], sign * (step + 1), 0, s if step == 3 else None, ALONG, s, step + 1))
                    for t, to in signs:
                        sends.append(put(b, xs[t], zrel, to, half, ACROSS, s, step, t))
                    p.task((PASS, b, l, ALONG, s, step), [(b, l, ALONG, s, step)], 0.03, sends)
                    far = put(b, xs[s], zrel, 2, half, ACROSS, s, step, 2)
                    p.task((PASS, b, l, ACROSS, s, step), [(b, l, ACROSS, s, step, s)], 0.03, [far])
        for s, sign in signs:
            p.task((PASS, U, l, ACROSS, s), [(U, l, ACROSS, s)], 0.03, [put(U, xs[s], 0, 2, s, ACROSS, s, 2)])
            sends = [put(U, zs[t], to, sign, None, ALONG, 1 + s, t, 1) for t, to in signs]
            p.task((PASS, U, l, ALONG, 1 + s), [(U, l, ACROSS, s)], 0.03, sends)
        sends = [put(U, zs[t], to, 2, None, ALONG, 3, t, 1) for t, to in signs]
        p.task((PASS, U, l, ALONG, 3), [(U, l, ACROSS, 0, 2), (U, l, ACROSS, 1, 2)], 0.03, sends)
        for column, xrel in enumerate((0, -1, 1, 2)):
            for t, sign in signs:
                for step in range(1, 4 if (t == 0) == (column in (0, 2)) else 3):
                    c = put(U, zs[t], sign * (step + 1), xrel, None, ALONG, column, t, step + 1)
                    p.task((PASS, U, l, ALONG, column, t, step), [(U, l, ALONG, column, t, step)], 0.03, [c])

    for k in range(NZ):
        c = p.copy((E, 0, GIVE, k), (YP, YM)[k % 2], 3.9, buf=E, layer=0, k=k)
        p.task((PASS, E, 0, GIVE, k), blocks[k], 0.05, [c])
        downs[0].extend([c, (PASS, E, 0, GIVE, k)])
    for cc in (0, 1):
        c = p.copy((E, 0, FAR, cc), YP, 3.9, buf=E, layer=0, far=cc)
        p.task((PASS, E, 0, FAR, cc), [(PASS, E, 0, GIVE, k) for k in range(NZ)] + [RELAY[cc]], 0.05, [c])
        downs[0].append((PASS, E, 0, FAR, cc))
    l, along = 1, {}
    for k in range(CHUNKS):
        for s, sign in signs:
            along[k, s] = p.copy((D, l, ALONG, k, s), zs[s], DOWN, buf=D, layer=l, kind=ALONG, chunk=k)
        sends = [along[k, 0], along[k, 1]]
        sends += [p.copy((D, l, ACROSS, k, s), xs[s], DOWN, buf=D, layer=l, kind=ACROSS, chunk=k, x=sign) for s, sign in signs]
        s = k % 2
        c = p.copy((D, l, ACROSS, k, 2), xs[s], DOWN, buf=D, layer=l, kind=ACROSS, chunk=k, x=2)
        for m in range(NZ // 2 + 1):
            needs = [(SOURCE, l)] if m == 0 else [along[k, 0], along[k, 1]]
            p.task((PASS, D, l, ALONG, k, m), needs, 0.05, sends, only=m)
            p.task((PASS, D, l, ACROSS, k, m), [(D, l, ACROSS, k, s)], 0.03, [c], only=m)
            downs[l].append((PASS, D, l, ALONG, k, m))
        downs[l].extend([sends[2], sends[3], c])
    p.task((SOURCE, l), [(D, l, OWN), GATE], 0.1, [], only=0)

    p.task((NORM,), [(START, 0)], 2.0, rank=1)
    p.task((HIDE, 0), [(NORM,)] + whole[0], 3.0, rank=1)
    p.task((GLUE, 0), downs[0], 0.8, rank=1)
    add_reduce(p, 0, [(HIDE, 0), (GLUE, 0)])
    for w in range(WAVES):
        for s, sign in signs:
            c = p.copy((N, w, CLOSE, s), (YP, YM)[s], ROWS / WAVES, buf=N, wave=w, y=sign, half=None, core=0)
            p.tasks[LAST, 0, w].sends.append(c)
            far = p.copy((N, w, FAR, s), (YP, YM)[s], ROWS / WAVES / 2, buf=N, wave=w, y=2, half=s, core=0)
            near = p.copy((N, w, PAIRED, s), PR, PAIR / WAVES, buf=N, wave=w, y=sign, half=None, core=1)
            p.task((PASS, N, w, CLOSE, s), [c], 0.03, [far, near])
            c = p.copy((N, w, PAIRED, FAR, s), PR, PAIR / WAVES / 2, buf=N, wave=w, y=2, half=s, core=1)
            p.task((PASS, N, w, FAR, s), [far], 0.03, [c])
        p.tasks[LAST, 0, w].sends.append(p.copy((N, w, PAIRED), PR, PAIR / WAVES, buf=N, wave=w, y=0, half=None, core=1))
        rows = {
            (0,): [(LAST, 0, w), (N, w, PAIRED)],
            (1, 3): [(N, w, CLOSE, 0), (N, w, PAIRED, 0), (N, w, CLOSE, 1), (N, w, PAIRED, 1)],
            (2,): [(N, w, FAR, 0), (N, w, FAR, 1), (N, w, PAIRED, FAR, 0), (N, w, PAIRED, FAR, 1)],
        }
        for rs in GROUPS[::-1]:
            p.task((HIDE, 1, w, rs), rows[rs] + whole[1], 1.2, rank=1)
    p.task((GLUE, 1), downs[1], 0.8, rank=1)
    add_reduce(p, 1, [(GLUE, 1)])
    for l in (0, 1):
        for buf in (G, U):
            for part in (0, 1):
                p.task((TURN, buf, l, part), whole[l] + [(HIDE, 0)], 0.5, rank=2)
    rank_copies(p)
    p.sequence = p.order()
    return p


def add_reduce(p, l, needs):
    for w in range(WAVES):
        for rs in GROUPS:
            c = [p.copy((R, l, w, PAIRED, r), PR, PAIR / WAVES, buf=R, layer=l, wave=w, kind=PAIRED, rel=r) for r in rs]
            p.task((PART, l, w, rs), needs + ([(HIDE, 1, w, rs)] if l else []), 0.7, c, rank=1)
        far, near = [
            [p.copy((R, l, w, kind, s), (YP, YM)[s], ROWS / WAVES / part, buf=R, layer=l, wave=w, kind=kind, side=s) for s in (0, 1)]
            for kind, part in ((FAR, 2), (CLOSE, 1))
        ]
        p.task((SUM, l, w, 2), [(PART, l, w, (2,)), (R, l, w, PAIRED, 2)], 0.15, far)
        for s, r in enumerate((1, 3)):
            p.task((SUM, l, w, r), [(PART, l, w, (1, 3)), (R, l, w, PAIRED, r), far[s]], 0.15, [near[s]])
        p.task((LAST, l, w), [(PART, l, w, (0,)), (R, l, w, PAIRED, 0)] + near, 0.4)


def normalized(rows):
    scale = lax.rsqrt(jnp.mean(rows * rows, axis=-1, keepdims=True) + 1e-06)
    return (rows * scale).astype(BF16)


def gated(normed, w_gate, w_up):
    gate = jnp.dot(normed, w_gate, preferred_element_type=F32)
    upper = jnp.dot(normed, w_up, preferred_element_type=F32)
    return (gate / (1.0 + jnp.exp(-gate)) * upper).astype(BF16)


def kernel(
    plan,
    prompt_hbm,
    gain_a, gate_a, up_a, down_a,
    gain_b, gate_b, up_b, down_b,
    gt0, ut0, t0, gt1, ut1, t1, mixed,
    prompt, normed, hidden, part, stream,
    g0, u0, g1, u1, squares, given, relayed, d1, stage,
    pair0, pair1, far0, far1, near0, near1, sums,
    gains, gates, depths,
    load_sem, send_sem, recv_sem, own_sem,
):
    gr, fs, tp = lax.axis_index("gr"), lax.axis_index("fs"), lax.axis_index("tp")
    z = gr * 4 + fs // 4
    x = lax.rem(fs, 4)
    y = tp // 2
    core = lax.rem(tp, 2)

    def device(xx, yy, zz, cc):
        return (zz // 4, lax.rem(zz, 4) * 4 + xx, yy * 2 + cc)

    def zat(k):
        return lax.rem(z + (k % NZ), NZ) if k % NZ else z

    def xat(k):
        return lax.rem(x + (k % NX), NX) if k % NX else x

    def yat(k):
        return lax.rem(y + (k % NY), NY) if k % NY else y

    other = 1 - core
    peers = {
        ZP: device(x, y, zat(1), core),
        ZM: device(x, y, zat(-1), core),
        XP: device(xat(1), y, z, core),
        XM: device(xat(-1), y, z, core),
        YP: device(x, yat(1), z, core),
        YM: device(x, yat(-1), z, core),
        PR: device(x, y, z, other),
    }
    weights = {(G, 0): g0, (U, 0): u0, (G, 1): g1, (U, 1): u1}
    turned = {(G, 0): gt0, (U, 0): ut0, (G, 1): gt1, (U, 1): ut1}
    talls = (t0, t1)
    pairs, fars, nears = (pair0, pair1), (far0, far1), (near0, near1)
    dist = lax.rem(z + NZ - tp, NZ)

    def rows_at(ref, row, half):
        if half is None:
            return ref.at[pl.ds(pl.multiple_of(row, 64), 64), :]
        return ref.at[pl.ds(pl.multiple_of(row + 32 * half, 32), 32), :]

    def refs(c, sender):
        dz, dx, dy = STEP[c.link] if sender else (0, 0, 0)
        at = c.at
        if c.buf == E:
            ref = squares.at[zat(at["z"] + dz) * NX + xat(at["x"] + dx)]
            if at["half"] is not None:
                ref = ref.at[:, pl.ds(128 * at["half"], 128)]
            return ref, ref
        if c.buf in (G, U):
            row = (zat(at["z"] + dz) * NX + xat(at["x"] + dx)) * 64
            ref = rows_at(weights[c.buf, at["layer"]], row, at["half"])
            return ref, ref
        if c.buf == D:
            n = 8 // CHUNKS
            ref = d1.at[xat(at.get("x", 0) + dx), pl.ds(at["chunk"] * n, n)]
            return ref, ref
        w = at["wave"]
        if c.buf == N:
            cc = other if at["core"] and not sender else core
            row, size = (yat(at["y"] + dy) * 2 + cc) * 64 + WAVE * w, WAVE
            if at["half"] is not None:
                row, size = row + WAVE // 2 * at["half"], WAVE // 2
            ref = normed.at[pl.ds(pl.multiple_of(row, WAVE // 2), size), :]
            return ref, ref
        l, wave = at["layer"], pl.ds(WAVE * w, WAVE)
        if at["kind"] == PAIRED:
            row = (yat(at["rel"]) * 2 + other) * 64 + WAVE * w
            return part.at[l, pl.ds(pl.multiple_of(row, WAVE), WAVE), :], pairs[l].at[at["rel"], wave, :]
        side = at["side"]
        if at["kind"] == FAR:
            half = WAVE // 2
            return sums.at[l, 2, pl.ds(WAVE * w + half * side, half), :], fars[l].at[side, pl.ds(half * w, half), :]
        return sums.at[l, 1 + 2 * side, wave, :], nears[l].at[side, wave, :]

    def describe(c, sender):
        src, dst = refs(c, sender)
        return pltpu.make_async_remote_copy(
            src_ref=src,
            dst_ref=dst,
            send_sem=send_sem.at[c.idx],
            recv_sem=recv_sem.at[c.idx],
            device_id=peers[c.link],
            device_id_type=MESH,
        )

    def own_copy(c, t):
        return pltpu.make_async_remote_copy(
            src_ref=stage,
            dst_ref=d1.at[x, t],
            send_sem=send_sem.at[c.idx],
            recv_sem=own_sem.at[1, t],
            device_id=device(x, z // 2, z, lax.rem(z, 2)),
            device_id_type=MESH,
        )

    onward, back = [lax.rem(y + 1 + 2 * cc, NY) for cc in (core, other)]

    def given_copy(c, t, way=False):
        to = zat(c.at["k"])
        return pltpu.make_async_remote_copy(
            src_ref=squares.at[pl.ds(to * NX, NX)],
            dst_ref=relayed.at[lax.rem(to, 2)] if way else given.at[t],
            send_sem=send_sem.at[c.idx],
            recv_sem=own_sem.at[2, lax.rem(to, 2)] if way else own_sem.at[0, t],
            device_id=(gr, fs, onward * 2 + core) if way else (gr, fs, to),
            device_id_type=MESH,
        )

    def far_copy(c):
        cc, t = c.at["far"], back * 2 + core
        return pltpu.make_async_remote_copy(
            src_ref=relayed.at[cc],
            dst_ref=given.at[t],
            send_sem=send_sem.at[c.idx],
            recv_sem=own_sem.at[0, t],
            device_id=(gr, fs, onward * 2 + cc),
            device_id_type=MESH,
        )

    def passes(c):
        if "k" in c.at:
            return zat(c.at["k"]) != tp
        if c.buf != D or c.at["kind"] == ACROSS:
            return None
        if c.at["kind"] == OWN:
            return dist != 0
        return dist < 4 if c.link == ZP else jnp.logical_or(dist == 0, dist > 5)

    def if_so(here, act):
        if here is None:
            act()
        else:
            pl.when(here)(act)

    def is_own(c):
        return c.buf == D and c.at["kind"] == OWN

    def outgoing(c):
        if "far" in c.at:
            return far_copy(c)
        return given_copy(c, tp) if "k" in c.at else own_copy(c, tp) if is_own(c) else describe(c, True)

    def send(c, here):
        if "k" in c.at:
            opposite = lax.rem(zat(c.at["k"]) // 2 + NY - y, NY) == 2
            if_so(opposite, given_copy(c, tp, True).start)
            here = jnp.logical_and(here, jnp.logical_not(opposite))
        if_so(here, outgoing(c).start)

    def sent(c):
        if_so(passes(c), outgoing(c).wait_send)

    seen = set()

    def arrived(key, only):
        c = plan.copies[key]
        if "k" in c.at:
            t = c.at["k"]
            if_so(tp != t, given_copy(c, t).wait_recv)
            return
        if c.buf == D and c.at["kind"] == ALONG:
            if_so(dist == (only if c.link == ZP else NZ - only), describe(c, False).wait_recv)
            return
        if (key, only) in seen or (only is None and (key, 4) in seen):
            return
        seen.add((key, only))
        if is_own(c):
            for t in range(8):
                if_so(jnp.logical_and(dist == 0, tp != t), own_copy(c, t).wait_recv)
            return
        here = None if only is None else hops == only
        if_so(here, describe(c, False).wait_recv)

    hops = jnp.minimum(dist, NZ - dist)
    eye = lax.broadcasted_iota(jnp.int32, (64, 64), 0) == lax.broadcasted_iota(jnp.int32, (64, 64), 1)

    def fold(gain, w):
        column = jnp.sum(jnp.where(eye, gain[...], 0.0), axis=1, keepdims=True)
        return (column * w[...]).astype(BF16)

    mine = pl.ds(pl.multiple_of((z * NX + x) * 64, 64), 64)

    def rows_of(r, cc, w):
        return pl.ds(pl.multiple_of((yat(r) * 2 + cc) * 64 + WAVE * w, WAVE), WAVE)

    def group(rs, w):
        return [rows_of(r, cc, w) for r in rs for cc in (0, 1)]

    loads = [
        pltpu.make_async_copy(src, dst, load_sem.at[i])
        for i, (src, dst) in enumerate(
            (
                (gain_a, gains.at[0]), (gate_a, gates.at[0]), (up_a, gates.at[1]), (down_a, depths.at[0]),
                (gain_b, gains.at[1]), (gate_b, gates.at[2]), (up_b, gates.at[3]), (down_b, depths.at[1]),
                (prompt_hbm, prompt),
            )
        )
    ]

    def begin():
        for load in loads:
            load.start()
        barrier = pltpu.get_barrier_semaphore()
        greet = [peers[k] for k in (ZP, ZM, XP, XM)]
        greet += [(gr, fs, lax.rem(tp + k, 8)) for k in range(1, 8)]
        for who in greet:
            pl.semaphore_signal(barrier, inc=1, device_id=who, device_id_type=MESH)
        for load in loads[:8]:
            load.wait()
        for i, ref in enumerate((g0, u0, g1, u1)):
            ref[mine, :] = fold(gains.at[i // 2], gates.at[i])
        squares[z * NX + x] = depths[0].astype(BF16)
        stage[...] = depths[1].astype(BF16)

        @pl.when(dist == 0)
        def _():
            d1[x, tp] = depths[1].astype(BF16)

        pl.semaphore_wait(barrier, len(greet))

    def norm():
        loads[8].wait()

        @pl.loop(0, 8)
        def _(i):
            at = pl.ds(pl.multiple_of(i * 64, 64), 64)
            normed[at, :] = normalized(prompt[at, :].astype(F32))

    def hide(l, w=None, rs=None):
        if l == 0:

            @pl.loop(0, 2)
            def _(i):
                at = pl.ds(pl.multiple_of(i * 256, 256), 256)
                hidden[at, :] = gated(normed[at, :], g0[...], u0[...])

            return
        spots = group(rs, w)
        out = gated(jnp.concatenate([normed[at, :] for at in spots], axis=0), g1[...], u1[...])
        for i, at in enumerate(spots):
            hidden[at, :] = out[WAVE * i : WAVE * (i + 1)]

    def turn(buf, l, piece):
        src, dst = weights[buf, l], turned[buf, l]

        @pl.loop(0, 4)
        def _(i):
            at = pl.ds(pl.multiple_of((piece * 4 + i) * 256, 256), 256)
            dst[:, at] = src[at, :].astype(F32).T.astype(BF16)

    def glue(l):
        if l == 0:
            for k in range(NX):
                given[tp, k] = squares[tp * NX + k]
        for t in range(8):
            blocks = [(given[t, k] if l == 0 else d1[k, t]).astype(F32) for k in range(NX)]
            rows = jnp.concatenate(blocks, axis=0)
            talls[l][:, 256 * t : 256 * (t + 1)] = rows.astype(BF16)

    def partial(l, w, rs):
        spots = group(rs, w)
        rows = jnp.concatenate([hidden[at, :] for at in spots], axis=0)
        out = jnp.dot(rows, talls[l][...], preferred_element_type=F32).astype(BF16)
        for i, at in enumerate(spots):
            part[l, at, :] = out[WAVE * i : WAVE * (i + 1)]

    def chip_sum(l, w, r):
        wave = slice(WAVE * w, WAVE * (w + 1))
        return part[l, rows_of(r, core, w), :].astype(F32) + pairs[l][r, wave, :].astype(F32)

    def add_up(l, w, r):
        total, half = chip_sum(l, w, r), WAVE // 2
        lower, upper = slice(WAVE * w, WAVE * w + half), slice(WAVE * w + half, WAVE * (w + 1))
        first, second = total[:half], total[half:]
        if r == 1:
            first = first + fars[l][0, half * w : half * (w + 1), :].astype(F32)
        if r == 3:
            second = second + fars[l][1, half * w : half * (w + 1), :].astype(F32)
        sums[l, r, lower, :] = first.astype(BF16)
        sums[l, r, upper, :] = second.astype(BF16)

    def last(l, w):
        wave = slice(WAVE * w, WAVE * (w + 1))
        total = chip_sum(l, w, 0) + nears[l][0, wave, :].astype(F32) + nears[l][1, wave, :].astype(F32)
        if l == 0:
            at = rows_of(0, core, w)
            rows = prompt[at, :].astype(F32) + 0.5 * total
            stream[wave, :] = rows
            normed[at, :] = normalized(rows)
        else:
            mixed[wave, :] = (stream[wave, :] + 0.5 * total).astype(BF16)

    work = {BEGIN: begin, NORM: norm, HIDE: hide, TURN: turn, GLUE: glue, PART: partial, SUM: add_up, LAST: last}
    for key, only in plan.sequence:
        if key in plan.copies:
            c = plan.copies[key]
            here = passes(c)
            if only is not None:
                here = hops == only if here is None else jnp.logical_and(here, hops == only)
            send(c, here)
            continue
        task = plan.tasks[key]
        for n in task.needs:
            if n in plan.copies and not (task.only == 4 and plan.copies[n].link == ZM and plan.copies[n].at.get("kind") == ALONG):
                arrived(n, task.only)
        if key[:2] == (PASS, E) and key[3] == FAR:
            cc = key[4]
            pltpu.make_async_remote_copy(
                src_ref=relayed.at[cc],
                dst_ref=relayed.at[cc],
                send_sem=send_sem.at[0],
                recv_sem=own_sem.at[2, cc],
                device_id=peers[PR],
                device_id_type=MESH,
            ).wait_recv()
        if key[0] in work:
            work[key[0]](*key[1:])
    for c in plan.copies.values():
        sent(c)


def hand_out(*refs):
    sources, targets, sem = refs[:7], refs[7:14], refs[14]
    copies = [pltpu.make_async_copy(a, b, sem.at[i]) for i, (a, b) in enumerate(zip(sources, targets))]
    for copy in copies:
        copy.start()
    for copy in copies:
        copy.wait()


def shards(prompt, gain_first, gate_first, up_first, down_first, gain_second, gate_second, up_second, down_second):
    plan = build_plan()
    rows, width = prompt.shape
    units = gate_first.shape[1]
    depth, columns = down_first.shape
    count = len(plan.copies)
    sem, vmem = pltpu.SemaphoreType.DMA, pltpu.VMEM
    block = rows // 8
    tall = jax.ShapeDtypeStruct((units, width), BF16)
    shapes = (tall,) * 6 + (jax.ShapeDtypeStruct((block, width), BF16),)
    outs = pl.pallas_call(
        functools.partial(kernel, plan),
        out_shape=shapes,
        in_specs=[pl.BlockSpec(memory_space=pltpu.HBM)] * 9,
        out_specs=(pl.BlockSpec(memory_space=vmem),) * 7,
        scratch_shapes=[
            vmem((rows, width), BF16),
            vmem((rows, width), BF16),
            vmem((rows, units), BF16),
            vmem((2, rows, width), BF16),
            vmem((block, width), F32),
            *[vmem((width, units), BF16)] * 4,
            vmem((NX * NZ, depth, columns), BF16),
            vmem((8, NX, depth, columns), BF16),
            vmem((2, NX, depth, columns), BF16),
            vmem((NX, 8, depth, columns), BF16),
            vmem((depth, columns), BF16),
            *[vmem((NY, block, width), BF16)] * 2,
            *[vmem((2, block // 2, width), BF16)] * 2,
            *[vmem((2, block, width), BF16)] * 2,
            vmem((2, NY, block, width), BF16),
            vmem((2, 1, gain_first.shape[0]), F32),
            vmem((4, *gate_first.shape), F32),
            vmem((2, depth, columns), F32),
            sem((9,)),
            sem((count,)),
            sem((count,)),
            sem((3, 8)),
        ],
        compiler_params=pltpu.CompilerParams(collective_id=0, has_side_effects=True, vmem_limit_bytes=LIMIT),
        name="handover",
    )(
        *[
            pltpu.with_memory_space_constraint(a, pltpu.HBM)
            for a in (
                prompt,
                gain_first.reshape(1, -1), gate_first, up_first, down_first,
                gain_second.reshape(1, -1), gate_second, up_second, down_second,
            )
        ],
    )
    outs = pl.pallas_call(
        hand_out,
        out_shape=shapes,
        in_specs=[pl.BlockSpec(memory_space=vmem)] * 7,
        out_specs=(pl.BlockSpec(memory_space=pl.ANY),) * 7,
        scratch_shapes=[sem((7,))],
        compiler_params=pltpu.CompilerParams(vmem_limit_bytes=16 * 1024 * 1024),
        name="hand_out",
    )(*outs)
    return (outs[0].T, outs[1].T, outs[2], outs[3].T, outs[4].T, outs[5], outs[6])


LIMIT = 44 * 1024 * 1024


def solution(mesh):
    rows = P(("gr", "fs"), None)
    block = P(("gr", "fs"), "tp")
    line = P(("gr", "fs"))
    return jax.shard_map(
        shards,
        mesh=mesh,
        in_specs=(rows, line, block, block, block, line, block, block, block),
        out_specs=(
            P(None, "tp"),
            P(None, "tp"),
            P("tp", None),
            P(None, "tp"),
            P(None, "tp"),
            P("tp", None),
            P(("gr", "fs", "tp"), None),
        ),
        check_vma=False,
    )
```

```python
import functools
import heapq

import jax
import jax.numpy as jnp
from jax import lax
from jax.experimental import pallas as pl
from jax.experimental.pallas import tpu as pltpu
from jax.sharding import PartitionSpec as P

MESH = pl.DeviceIdType.MESH
F32, BF16 = jnp.float32, jnp.bfloat16
NX, NY, NZ = 4, 4, 8
CHUNKS = 4
WAVES = 2
WAVE = 64 // WAVES
GROUPS = ((2,), (1, 3), (0,))

UNIT, SQUARE, DOWN, ROWS, PAIR, WIRE, NEAR = 1.15, 1.05, 2.1, 5.7, 0.5, 2.1, 1.0

ZP, ZM, XP, XM, YP, YM, PR = LINKS = range(7)
STEP = {ZP: (1, 0, 0), ZM: (-1, 0, 0), XP: (0, 1, 0), XM: (0, -1, 0), YP: (0, 0, 1), YM: (0, 0, -1), PR: (0, 0, 0)}
G, U, D, N, R, E = range(6)
BEGIN, START, NORM, HIDE, GLUE, TURN, PART, SUM, LAST, SOURCE, PASS = range(100, 111)
OWN, ALONG, ACROSS, PAIRED, FAR, CLOSE, GIVE = range(200, 207)


class Copy:
    def __init__(self, idx, link, dur, at):
        self.idx, self.link, self.dur = idx, link, dur
        self.buf = at["buf"]
        self.at = at
        self.rank = 0


class Task:
    def __init__(self, needs, dur, sends, rank, only):
        self.needs, self.dur, self.sends, self.rank, self.only = list(needs), dur, list(sends), rank, only

    def falls_to(self, d):
        return self.only is None or min(d, NZ - d) == self.only


class Plan:
    def __init__(self):
        self.copies, self.tasks = {}, {}

    def copy(self, key, link, dur, **at):
        self.copies[key] = Copy(len(self.copies), link, dur, at)
        return key

    def task(self, key, needs, dur, sends=(), rank=0, only=None):
        self.tasks[key] = Task(needs, dur, sends, rank, only)

    def starts_here(self, c, d):
        if c.buf != D or c.at["kind"] == ACROSS:
            return True
        if c.at["kind"] == OWN:
            return d != 0
        return d < 4 if c.link == ZP else d == 0 or d > 5

    def absent(self, need, d):
        if need in self.tasks:
            return not self.tasks[need].falls_to(d)
        copy = self.copies.get(need)
        if copy is None or copy.buf != D:
            return False
        if copy.at["kind"] == OWN:
            return d != 0
        return copy.at["kind"] == ALONG and (d == 0 or (copy.link == ZP) != (d < 5))

    def simulate(self, fixed=None):
        kinds = [(d, c) for d in range(NZ) for c in range(2)]
        left = {k: {t: {n for n in v.needs if not self.absent(n, k[0])} for t, v in self.tasks.items() if v.falls_to(k[0])} for k in kinds}
        users = {}
        for t, v in self.tasks.items():
            for n in v.needs:
                users.setdefault(n, []).append(t)
        place = {t: i for i, t in enumerate(self.tasks)}
        ready, pending, turn = {k: [] for k in kinds}, {}, {k: 0 for k in kinds}
        free, busy = {}, {k: 0.0 for k in kinds}
        starts = {k: {} for k in kinds}
        events, self.count = [], 0

        def at_time(at, k, link, what):
            self.count += 1
            heapq.heappush(events, (at, self.count, k, link, what))

        def enable(k, t, at):
            rank = self.tasks[t].rank
            heapq.heappush(ready[k], (rank, place[t] if rank else at, place[t], t))

        def start(k, key, only, now):
            copy = self.copies[key]
            d, c = k
            starts[k][key, only] = now
            end = free[k, copy.link] = max(now, free.get((k, copy.link), 0.0)) + copy.dur
            dz, _, dy = STEP[copy.link]
            to = ((d + dz - 2 * dy) % NZ, c)
            if copy.buf == D and copy.at["kind"] == OWN:
                to = (0, c)
            if copy.link == PR:
                to = ((d + (-1 if c == 0 else 1)) % NZ, 1 - c)
            at_time(end + (NEAR if copy.link == PR else WIRE), to, None, key)

        for k in kinds:
            for t in left[k]:
                if not left[k][t]:
                    enable(k, t, 0.0)
            at_time(0.0, k, None, None)
        while events:
            now, _, k, link, what = heapq.heappop(events)
            if link is not None:
                queue = pending[k, link]
                if queue and now >= free.get((k, link), 0.0) - ahead(queue[0][0]) - 1e-9:
                    _, _, key, only = heapq.heappop(queue)
                    start(k, key, only, now)
                if queue:
                    at_time(max(now, free.get((k, link), 0.0) - ahead(queue[0][0])), k, link, None)
                continue
            for t in users.get(what, ()) if what is not None else ():
                if what in left[k].get(t, ()):
                    left[k][t].discard(what)
                    if not left[k][t]:
                        enable(k, t, now)
            if what in self.tasks and fixed is None:
                task = self.tasks[what]
                for key in task.sends:
                    copy = self.copies[key]
                    if self.starts_here(copy, k[0]):
                        self.count += 1
                        heapq.heappush(pending.setdefault((k, copy.link), []), (copy.rank, self.count, key, task.only))
                        at_time(max(now, free.get((k, copy.link), 0.0) - ahead(copy.rank)), k, copy.link, None)
            if now < busy[k]:
                continue
            if fixed is None:
                if not ready[k]:
                    continue
                t = heapq.heappop(ready[k])[3]
            else:
                t = None
                while turn[k] < len(fixed):
                    key, only = fixed[turn[k]]
                    if key in self.tasks:
                        if key in left[k]:
                            if not left[k][key]:
                                t = key
                                turn[k] += 1
                            break
                    elif (only is None or min(k[0], NZ - k[0]) == only) and self.starts_here(self.copies[key], k[0]):
                        start(k, key, only, now)
                    turn[k] += 1
                if t is None:
                    continue
            starts[k][t, None] = now
            busy[k] = now + self.tasks[t].dur
            at_time(busy[k], k, None, t)
        if fixed is not None and any(turn[k] < len(fixed) for k in kinds):
            return starts, 1e9
        return starts, max(busy.values())

    def find_before(self):
        starters, self.before = {}, {}
        for t, v in self.tasks.items():
            for c in v.sends:
                starters.setdefault(c, []).append((c, v.only))
                self.before[c, v.only] = [(t, None)]
        for t, v in self.tasks.items():
            before = [(n, None) for n in v.needs if n in self.tasks]
            for n in v.needs:
                for c, m in starters.get(n, ()):
                    hop = self.copies[n].buf == D and self.copies[n].at["kind"] == ALONG
                    if m is None or v.only is None or m == v.only - hop:
                        before.append((c, m))
            self.before[t, None] = before

    def line_up(self, starts, mix):
        at = {}
        for e in self.before:
            here = [v[e] for v in starts.values() if e in v]
            at[e] = mix * max(here) + (1 - mix) * sum(here) / len(here) if here else 0.0
        place = {e: i for i, e in enumerate(self.before)}
        changed = True
        while changed:
            changed = False
            for e, before in self.before.items():
                for n in before:
                    if at[n] >= at[e]:
                        at[e] = at[n] + 1e-6
                        changed = True
        return sorted(self.before, key=lambda e: (at[e], place[e]))

    def order(self):
        self.find_before()
        starts, self.ideal = self.simulate()
        best = None
        for mix in (0.0, 0.2, 0.4, 0.6, 0.8, 1.0):
            line = self.line_up(starts, mix)
            total = self.simulate(line)[1]
            if best is None or total < best[0]:
                best = total, line
        self.total = best[0]
        return best[1]


GIVEN = 4.5
GATE = (PASS, E, 0, ALONG, 0, 1)
RELAY = [(E, 0, GIVE, 4)] * 2
AHEAD = 1.0
RANKS = [0, 0, -3, 23, 1, 3, 18, 20, 29, 34, 31, 37, 30, -50]


def ahead(rank):
    return AHEAD if rank >= 0 else 9.0


def rank_copies(p):
    for key, c in p.copies.items():
        if c.buf not in (G, U, D, E):
            continue
        l = c.at["layer"]
        if c.link in (YP, YM):
            r = 0
        elif c.link in (ZP, ZM):
            if c.buf == D:
                r = RANKS[0]
            elif c.buf in (G, E):
                r = RANKS[1] + RANKS[2] * key[-1]
            else:
                r = RANKS[3] + RANKS[4] * key[-1]
        elif c.buf == U:
            r = RANKS[5] if len(key) == 4 else RANKS[6]
        elif c.buf in (G, E):
            far = c.at["x"] == 2
            r = RANKS[9] if far else RANKS[7] if key[2] == OWN else RANKS[8]
        else:
            r = RANKS[11] if c.at["x"] == 2 else RANKS[10]
        c.rank = r + RANKS[12] * l + RANKS[13] * (c.buf == E)


def build_plan():
    p = Plan()
    whole, downs, blocks = ([], []), ([], []), {}
    signs = ((0, -1), (1, 1))
    zs, xs = (ZP, ZM), (XP, XM)

    p.task((BEGIN,), [], 3.0, [p.copy((D, 1, OWN), YP, 2.0, buf=D, layer=1, kind=OWN)])
    for l in (0, 1):

        def put(buf, link, zrel, xrel, half, *tag):
            key = (buf, l, *tag)
            unit = SQUARE if buf == E else UNIT
            p.copy(key, link, unit * (1.0 if half is None else 0.5), buf=buf, layer=l, z=zrel, x=xrel, half=half)
            (blocks.setdefault(zrel % NZ, []) if buf == E else whole[l]).append(key)
            return key

        z_first = (G, E) if l == 0 else (G,)
        first = []
        for s, sign in signs:
            first += [put(b, zs[s], sign, 0, None, ALONG, s, 1) for b in z_first]
            first += [put(U, xs[s], 0, sign, None, ACROSS, s)]
            first += [put(U, zs[s], sign, 0, None, ALONG, 0, s, 1)]
            first += [put(b, xs[s], 0, sign, None, OWN, s) for b in z_first]
        p.task((START, l), [(BEGIN,)] if l == 0 else [(START, 0)], 0.2, first)

        for b in z_first:
            for s, sign in signs:
                p.task((PASS, b, l, OWN, s), [(b, l, OWN, s)], 0.03, [put(b, xs[s], 0, 2, s, OWN, s, 2)])
                for step in (1, 2, 3, 4):
                    zrel, half = sign * step, s if step == 4 else None
                    sends = []
                    if step < 4:
                        sends.append(put(b, zs[s], sign * (step + 1), 0, s if step == 3 else None, ALONG, s, step + 1))
                    for t, to in signs:
                        sends.append(put(b, xs[t], zrel, to, half, ACROSS, s, step, t))
                    p.task((PASS, b, l, ALONG, s, step), [(b, l, ALONG, s, step)], 0.03, sends)
                    far = put(b, xs[s], zrel, 2, half, ACROSS, s, step, 2)
                    p.task((PASS, b, l, ACROSS, s, step), [(b, l, ACROSS, s, step, s)], 0.03, [far])
        for s, sign in signs:
            p.task((PASS, U, l, ACROSS, s), [(U, l, ACROSS, s)], 0.03, [put(U, xs[s], 0, 2, s, ACROSS, s, 2)])
            sends = [put(U, zs[t], to, sign, None, ALONG, 1 + s, t, 1) for t, to in signs]
            p.task((PASS, U, l, ALONG, 1 + s), [(U, l, ACROSS, s)], 0.03, sends)
        sends = [put(U, zs[t], to, 2, None, ALONG, 3, t, 1) for t, to in signs]
        p.task((PASS, U, l, ALONG, 3), [(U, l, ACROSS, 0, 2), (U, l, ACROSS, 1, 2)], 0.03, sends)
        for column, xrel in enumerate((0, -1, 1, 2)):
            for t, sign in signs:
                for step in range(1, 4 if (t == 0) == (column in (0, 2)) else 3):
                    c = put(U, zs[t], sign * (step + 1), xrel, None, ALONG, column, t, step + 1)
                    p.task((PASS, U, l, ALONG, column, t, step), [(U, l, ALONG, column, t, step)], 0.03, [c])

    for k in range(NZ):
        c = p.copy((E, 0, GIVE, k), (YP, YM)[k % 2], GIVEN, buf=E, layer=0, k=k)
        p.task((PASS, E, 0, GIVE, k), blocks[k], 0.05, [c])
        downs[0].extend([c, (PASS, E, 0, GIVE, k)])
    for cc in (0, 1):
        c = p.copy((E, 0, FAR, cc), (YP, YM)[cc], GIVEN, buf=E, layer=0, far=cc)
        p.task((PASS, E, 0, FAR, cc), [(PASS, E, 0, GIVE, k) for k in range(NZ)] + [RELAY[cc]], 0.05, [c])
        downs[0].append((PASS, E, 0, FAR, cc))
    l, along = 1, {}
    for k in range(CHUNKS):
        for s, sign in signs:
            along[k, s] = p.copy((D, l, ALONG, k, s), zs[s], DOWN, buf=D, layer=l, kind=ALONG, chunk=k)
        sends = [along[k, 0], along[k, 1]]
        sends += [p.copy((D, l, ACROSS, k, s), xs[s], DOWN, buf=D, layer=l, kind=ACROSS, chunk=k, x=sign) for s, sign in signs]
        s = k % 2
        c = p.copy((D, l, ACROSS, k, 2), xs[s], DOWN, buf=D, layer=l, kind=ACROSS, chunk=k, x=2)
        for m in range(NZ // 2 + 1):
            needs = [(SOURCE, l)] if m == 0 else [along[k, 0], along[k, 1]]
            p.task((PASS, D, l, ALONG, k, m), needs, 0.05, sends, only=m)
            p.task((PASS, D, l, ACROSS, k, m), [(D, l, ACROSS, k, s)], 0.03, [c], only=m)
            downs[l].append((PASS, D, l, ALONG, k, m))
        downs[l].extend([sends[2], sends[3], c])
    p.task((SOURCE, l), [(D, l, OWN), GATE], 0.1, [], only=0)

    p.task((NORM,), [(START, 0)], 2.0, rank=1)
    p.task((HIDE, 0), [(NORM,)] + whole[0], 3.0, rank=1)
    p.task((GLUE, 0), downs[0], 0.8, rank=1)
    add_reduce(p, 0, [(HIDE, 0), (GLUE, 0)])
    for w in range(WAVES):
        for s, sign in signs:
            c = p.copy((N, w, CLOSE, s), (YP, YM)[s], ROWS / WAVES, buf=N, wave=w, y=sign, half=None, core=0)
            p.tasks[LAST, 0, w].sends.append(c)
            far = p.copy((N, w, FAR, s), (YP, YM)[s], ROWS / WAVES / 2, buf=N, wave=w, y=2, half=s, core=0)
            near = p.copy((N, w, PAIRED, s), PR, PAIR / WAVES, buf=N, wave=w, y=sign, half=None, core=1)
            p.task((PASS, N, w, CLOSE, s), [c], 0.03, [far, near])
            c = p.copy((N, w, PAIRED, FAR, s), PR, PAIR / WAVES / 2, buf=N, wave=w, y=2, half=s, core=1)
            p.task((PASS, N, w, FAR, s), [far], 0.03, [c])
        p.tasks[LAST, 0, w].sends.append(p.copy((N, w, PAIRED), PR, PAIR / WAVES, buf=N, wave=w, y=0, half=None, core=1))
        rows = {
            (0,): [(LAST, 0, w), (N, w, PAIRED)],
            (1, 3): [(N, w, CLOSE, 0), (N, w, PAIRED, 0), (N, w, CLOSE, 1), (N, w, PAIRED, 1)],
            (2,): [(N, w, FAR, 0), (N, w, FAR, 1), (N, w, PAIRED, FAR, 0), (N, w, PAIRED, FAR, 1)],
        }
        for rs in GROUPS[::-1]:
            p.task((HIDE, 1, w, rs), rows[rs] + whole[1], 1.2, rank=1)
    p.task((GLUE, 1), downs[1], 0.8, rank=1)
    add_reduce(p, 1, [(GLUE, 1)])
    for l in (0, 1):
        for buf in (G, U):
            for part in (0, 1):
                p.task((TURN, buf, l, part), whole[l] + [(HIDE, 0)], 0.5, rank=2)
    rank_copies(p)
    p.sequence = p.order()
    return p


def add_reduce(p, l, needs):
    for w in range(WAVES):
        for rs in GROUPS:
            c = [p.copy((R, l, w, PAIRED, r), PR, PAIR / WAVES, buf=R, layer=l, wave=w, kind=PAIRED, rel=r) for r in rs]
            p.task((PART, l, w, rs), needs + ([(HIDE, 1, w, rs)] if l else []), 0.7, c, rank=1)
        far, near = [
            [p.copy((R, l, w, kind, s), (YP, YM)[s], ROWS / WAVES / part, buf=R, layer=l, wave=w, kind=kind, side=s) for s in (0, 1)]
            for kind, part in ((FAR, 2), (CLOSE, 1))
        ]
        p.task((SUM, l, w, 2), [(PART, l, w, (2,)), (R, l, w, PAIRED, 2)], 0.15, far)
        for s, r in enumerate((1, 3)):
            p.task((SUM, l, w, r), [(PART, l, w, (1, 3)), (R, l, w, PAIRED, r), far[s]], 0.15, [near[s]])
        p.task((LAST, l, w), [(PART, l, w, (0,)), (R, l, w, PAIRED, 0)] + near, 0.4)


def normalized(rows):
    scale = lax.rsqrt(jnp.mean(rows * rows, axis=-1, keepdims=True) + 1e-06)
    return (rows * scale).astype(BF16)


def gated(normed, w_gate, w_up):
    gate = jnp.dot(normed, w_gate, preferred_element_type=F32)
    upper = jnp.dot(normed, w_up, preferred_element_type=F32)
    return (gate / (1.0 + jnp.exp(-gate)) * upper).astype(BF16)


def kernel(
    plan,
    prompt_hbm,
    gain_a, gate_a, up_a, down_a,
    gain_b, gate_b, up_b, down_b,
    gt0, ut0, t0, gt1, ut1, t1, mixed,
    prompt, normed, hidden, part, stream,
    g0, u0, g1, u1, squares, given, relayed, d1, stage,
    pair0, pair1, far0, far1, near0, near1, sums,
    gains, gates, depths,
    load_sem, send_sem, recv_sem, own_sem,
):
    gr, fs, tp = lax.axis_index("gr"), lax.axis_index("fs"), lax.axis_index("tp")
    z = gr * 4 + fs // 4
    x = lax.rem(fs, 4)
    y = tp // 2
    core = lax.rem(tp, 2)

    def device(xx, yy, zz, cc):
        return (zz // 4, lax.rem(zz, 4) * 4 + xx, yy * 2 + cc)

    def zat(k):
        return lax.rem(z + (k % NZ), NZ) if k % NZ else z

    def xat(k):
        return lax.rem(x + (k % NX), NX) if k % NX else x

    def yat(k):
        return lax.rem(y + (k % NY), NY) if k % NY else y

    other = 1 - core
    peers = {
        ZP: device(x, y, zat(1), core),
        ZM: device(x, y, zat(-1), core),
        XP: device(xat(1), y, z, core),
        XM: device(xat(-1), y, z, core),
        YP: device(x, yat(1), z, core),
        YM: device(x, yat(-1), z, core),
        PR: device(x, y, z, other),
    }
    weights = {(G, 0): g0, (U, 0): u0, (G, 1): g1, (U, 1): u1}
    turned = {(G, 0): gt0, (U, 0): ut0, (G, 1): gt1, (U, 1): ut1}
    talls = (t0, t1)
    pairs, fars, nears = (pair0, pair1), (far0, far1), (near0, near1)
    dist = lax.rem(z + NZ - tp, NZ)

    def rows_at(ref, row, half):
        if half is None:
            return ref.at[pl.ds(pl.multiple_of(row, 64), 64), :]
        return ref.at[pl.ds(pl.multiple_of(row + 32 * half, 32), 32), :]

    def refs(c, sender):
        dz, dx, dy = STEP[c.link] if sender else (0, 0, 0)
        at = c.at
        if c.buf == E:
            ref = squares.at[zat(at["z"] + dz) * NX + xat(at["x"] + dx)]
            if at["half"] is not None:
                ref = ref.at[:, pl.ds(128 * at["half"], 128)]
            return ref, ref
        if c.buf in (G, U):
            row = (zat(at["z"] + dz) * NX + xat(at["x"] + dx)) * 64
            ref = rows_at(weights[c.buf, at["layer"]], row, at["half"])
            return ref, ref
        if c.buf == D:
            n = 8 // CHUNKS
            ref = d1.at[xat(at.get("x", 0) + dx), pl.ds(at["chunk"] * n, n)]
            return ref, ref
        w = at["wave"]
        if c.buf == N:
            cc = other if at["core"] and not sender else core
            row, size = (yat(at["y"] + dy) * 2 + cc) * 64 + WAVE * w, WAVE
            if at["half"] is not None:
                row, size = row + WAVE // 2 * at["half"], WAVE // 2
            ref = normed.at[pl.ds(pl.multiple_of(row, WAVE // 2), size), :]
            return ref, ref
        l, wave = at["layer"], pl.ds(WAVE * w, WAVE)
        if at["kind"] == PAIRED:
            row = (yat(at["rel"]) * 2 + other) * 64 + WAVE * w
            return part.at[l, pl.ds(pl.multiple_of(row, WAVE), WAVE), :], pairs[l].at[at["rel"], wave, :]
        side = at["side"]
        if at["kind"] == FAR:
            half = WAVE // 2
            return sums.at[l, 2, pl.ds(WAVE * w + half * side, half), :], fars[l].at[side, pl.ds(half * w, half), :]
        return sums.at[l, 1 + 2 * side, wave, :], nears[l].at[side, wave, :]

    def describe(c, sender):
        src, dst = refs(c, sender)
        return pltpu.make_async_remote_copy(
            src_ref=src,
            dst_ref=dst,
            send_sem=send_sem.at[c.idx],
            recv_sem=recv_sem.at[c.idx],
            device_id=peers[c.link],
            device_id_type=MESH,
        )

    def own_copy(c, t):
        return pltpu.make_async_remote_copy(
            src_ref=stage,
            dst_ref=d1.at[x, t],
            send_sem=send_sem.at[c.idx],
            recv_sem=own_sem.at[1, t],
            device_id=device(x, z // 2, z, lax.rem(z, 2)),
            device_id_type=MESH,
        )

    onward, back = [lax.rem(y + 1 + 2 * cc, NY) for cc in (core, other)]

    def given_copy(c, t, way=False):
        to = zat(c.at["k"])
        return pltpu.make_async_remote_copy(
            src_ref=squares.at[pl.ds(to * NX, NX)],
            dst_ref=relayed.at[lax.rem(to, 2)] if way else given.at[t],
            send_sem=send_sem.at[c.idx],
            recv_sem=own_sem.at[2, lax.rem(to, 2)] if way else own_sem.at[0, t],
            device_id=(gr, fs, onward * 2 + core) if way else (gr, fs, to),
            device_id_type=MESH,
        )

    def far_copy(c):
        cc, t = c.at["far"], back * 2 + core
        return pltpu.make_async_remote_copy(
            src_ref=relayed.at[cc],
            dst_ref=given.at[t],
            send_sem=send_sem.at[c.idx],
            recv_sem=own_sem.at[0, t],
            device_id=(gr, fs, onward * 2 + cc),
            device_id_type=MESH,
        )

    def passes(c):
        if "k" in c.at:
            return zat(c.at["k"]) != tp
        if c.buf != D or c.at["kind"] == ACROSS:
            return None
        if c.at["kind"] == OWN:
            return dist != 0
        return dist < 4 if c.link == ZP else jnp.logical_or(dist == 0, dist > 5)

    def if_so(here, act):
        if here is None:
            act()
        else:
            pl.when(here)(act)

    def is_own(c):
        return c.buf == D and c.at["kind"] == OWN

    def outgoing(c):
        if "far" in c.at:
            return far_copy(c)
        return given_copy(c, tp) if "k" in c.at else own_copy(c, tp) if is_own(c) else describe(c, True)

    def send(c, here):
        if "k" in c.at:
            opposite = lax.rem(zat(c.at["k"]) // 2 + NY - y, NY) == 2
            if_so(opposite, given_copy(c, tp, True).start)
            here = jnp.logical_and(here, jnp.logical_not(opposite))
        if_so(here, outgoing(c).start)

    def sent(c):
        if_so(passes(c), outgoing(c).wait_send)

    seen = set()

    def arrived(key, only):
        c = plan.copies[key]
        if "k" in c.at:
            t = c.at["k"]
            if_so(tp != t, given_copy(c, t).wait_recv)
            return
        if c.buf == D and c.at["kind"] == ALONG:
            if_so(dist == (only if c.link == ZP else NZ - only), describe(c, False).wait_recv)
            return
        if (key, only) in seen or (only is None and (key, 4) in seen):
            return
        seen.add((key, only))
        if is_own(c):
            for t in range(8):
                if_so(jnp.logical_and(dist == 0, tp != t), own_copy(c, t).wait_recv)
            return
        here = None if only is None else hops == only
        if_so(here, describe(c, False).wait_recv)

    hops = jnp.minimum(dist, NZ - dist)
    eye = lax.broadcasted_iota(jnp.int32, (64, 64), 0) == lax.broadcasted_iota(jnp.int32, (64, 64), 1)

    def fold(gain, w):
        column = jnp.sum(jnp.where(eye, gain[...], 0.0), axis=1, keepdims=True)
        return (column * w[...]).astype(BF16)

    mine = pl.ds(pl.multiple_of((z * NX + x) * 64, 64), 64)

    def rows_of(r, cc, w):
        return pl.ds(pl.multiple_of((yat(r) * 2 + cc) * 64 + WAVE * w, WAVE), WAVE)

    def group(rs, w):
        return [rows_of(r, cc, w) for r in rs for cc in (0, 1)]

    loads = [
        pltpu.make_async_copy(src, dst, load_sem.at[i])
        for i, (src, dst) in enumerate(
            (
                (gain_a, gains.at[0]), (gate_a, gates.at[0]), (up_a, gates.at[1]), (down_a, depths.at[0]),
                (gain_b, gains.at[1]), (gate_b, gates.at[2]), (up_b, gates.at[3]), (down_b, depths.at[1]),
                (prompt_hbm, prompt),
            )
        )
    ]

    def begin():
        for load in loads:
            load.start()
        barrier = pltpu.get_barrier_semaphore()
        greet = [peers[k] for k in (ZP, ZM, XP, XM)]
        greet += [(gr, fs, lax.rem(tp + k, 8)) for k in range(1, 8)]
        for who in greet:
            pl.semaphore_signal(barrier, inc=1, device_id=who, device_id_type=MESH)
        for load in loads[:8]:
            load.wait()
        for i, ref in enumerate((g0, u0, g1, u1)):
            ref[mine, :] = fold(gains.at[i // 2], gates.at[i])
        squares[z * NX + x] = depths[0].astype(BF16)
        stage[...] = depths[1].astype(BF16)

        @pl.when(dist == 0)
        def _():
            d1[x, tp] = depths[1].astype(BF16)

        pl.semaphore_wait(barrier, len(greet))

    def norm():
        loads[8].wait()

        @pl.loop(0, 8)
        def _(i):
            at = pl.ds(pl.multiple_of(i * 64, 64), 64)
            normed[at, :] = normalized(prompt[at, :].astype(F32))

    def hide(l, w=None, rs=None):
        if l == 0:

            @pl.loop(0, 2)
            def _(i):
                at = pl.ds(pl.multiple_of(i * 256, 256), 256)
                hidden[at, :] = gated(normed[at, :], g0[...], u0[...])

            return
        spots = group(rs, w)
        out = gated(jnp.concatenate([normed[at, :] for at in spots], axis=0), g1[...], u1[...])
        for i, at in enumerate(spots):
            hidden[at, :] = out[WAVE * i : WAVE * (i + 1)]

    def turn(buf, l, piece):
        src, dst = weights[buf, l], turned[buf, l]

        @pl.loop(0, 4)
        def _(i):
            at = pl.ds(pl.multiple_of((piece * 4 + i) * 256, 256), 256)
            dst[:, at] = src[at, :].astype(F32).T.astype(BF16)

    def glue(l):
        if l == 0:
            for k in range(NX):
                given[tp, k] = squares[tp * NX + k]
        for t in range(8):
            blocks = [(given[t, k] if l == 0 else d1[k, t]).astype(F32) for k in range(NX)]
            rows = jnp.concatenate(blocks, axis=0)
            talls[l][:, 256 * t : 256 * (t + 1)] = rows.astype(BF16)

    def partial(l, w, rs):
        spots = group(rs, w)
        rows = jnp.concatenate([hidden[at, :] for at in spots], axis=0)
        out = jnp.dot(rows, talls[l][...], preferred_element_type=F32).astype(BF16)
        for i, at in enumerate(spots):
            part[l, at, :] = out[WAVE * i : WAVE * (i + 1)]

    def chip_sum(l, w, r):
        wave = slice(WAVE * w, WAVE * (w + 1))
        return part[l, rows_of(r, core, w), :].astype(F32) + pairs[l][r, wave, :].astype(F32)

    def add_up(l, w, r):
        total, half = chip_sum(l, w, r), WAVE // 2
        lower, upper = slice(WAVE * w, WAVE * w + half), slice(WAVE * w + half, WAVE * (w + 1))
        first, second = total[:half], total[half:]
        if r == 1:
            first = first + fars[l][0, half * w : half * (w + 1), :].astype(F32)
        if r == 3:
            second = second + fars[l][1, half * w : half * (w + 1), :].astype(F32)
        sums[l, r, lower, :] = first.astype(BF16)
        sums[l, r, upper, :] = second.astype(BF16)

    def last(l, w):
        wave = slice(WAVE * w, WAVE * (w + 1))
        total = chip_sum(l, w, 0) + nears[l][0, wave, :].astype(F32) + nears[l][1, wave, :].astype(F32)
        if l == 0:
            at = rows_of(0, core, w)
            rows = prompt[at, :].astype(F32) + 0.5 * total
            stream[wave, :] = rows
            normed[at, :] = normalized(rows)
        else:
            mixed[wave, :] = (stream[wave, :] + 0.5 * total).astype(BF16)

    work = {BEGIN: begin, NORM: norm, HIDE: hide, TURN: turn, GLUE: glue, PART: partial, SUM: add_up, LAST: last}
    for key, only in plan.sequence:
        if key in plan.copies:
            c = plan.copies[key]
            here = passes(c)
            if only is not None:
                here = hops == only if here is None else jnp.logical_and(here, hops == only)
            send(c, here)
            continue
        task = plan.tasks[key]
        for n in task.needs:
            if key[:2] == (PASS, E) and key[3] == FAR:
                continue
            if n in plan.copies and not (task.only == 4 and plan.copies[n].link == ZM and plan.copies[n].at.get("kind") == ALONG):
                arrived(n, task.only)
        if key[:2] == (PASS, E) and key[3] == FAR:
            cc = key[4]
            pltpu.make_async_remote_copy(
                src_ref=relayed.at[cc],
                dst_ref=relayed.at[cc],
                send_sem=send_sem.at[0],
                recv_sem=own_sem.at[2, cc],
                device_id=peers[PR],
                device_id_type=MESH,
            ).wait_recv()
        if key[0] in work:
            work[key[0]](*key[1:])
    for c in plan.copies.values():
        sent(c)


def hand_out(*refs):
    sources, targets, sem = refs[:7], refs[7:14], refs[14]
    copies = [pltpu.make_async_copy(a, b, sem.at[i]) for i, (a, b) in enumerate(zip(sources, targets))]
    for copy in copies:
        copy.start()
    for copy in copies:
        copy.wait()


def shards(prompt, gain_first, gate_first, up_first, down_first, gain_second, gate_second, up_second, down_second):
    plan = build_plan()
    rows, width = prompt.shape
    units = gate_first.shape[1]
    depth, columns = down_first.shape
    count = len(plan.copies)
    sem, vmem = pltpu.SemaphoreType.DMA, pltpu.VMEM
    block = rows // 8
    tall = jax.ShapeDtypeStruct((units, width), BF16)
    shapes = (tall,) * 6 + (jax.ShapeDtypeStruct((block, width), BF16),)
    outs = pl.pallas_call(
        functools.partial(kernel, plan),
        out_shape=shapes,
        in_specs=[pl.BlockSpec(memory_space=pltpu.HBM)] * 9,
        out_specs=(pl.BlockSpec(memory_space=vmem),) * 7,
        scratch_shapes=[
            vmem((rows, width), BF16),
            vmem((rows, width), BF16),
            vmem((rows, units), BF16),
            vmem((2, rows, width), BF16),
            vmem((block, width), F32),
            *[vmem((width, units), BF16)] * 4,
            vmem((NX * NZ, depth, columns), BF16),
            vmem((8, NX, depth, columns), BF16),
            vmem((2, NX, depth, columns), BF16),
            vmem((NX, 8, depth, columns), BF16),
            vmem((depth, columns), BF16),
            *[vmem((NY, block, width), BF16)] * 2,
            *[vmem((2, block // 2, width), BF16)] * 2,
            *[vmem((2, block, width), BF16)] * 2,
            vmem((2, NY, block, width), BF16),
            vmem((2, 1, gain_first.shape[0]), F32),
            vmem((4, *gate_first.shape), F32),
            vmem((2, depth, columns), F32),
            sem((9,)),
            sem((count,)),
            sem((count,)),
            sem((3, 8)),
        ],
        compiler_params=pltpu.CompilerParams(collective_id=0, has_side_effects=True, vmem_limit_bytes=LIMIT),
        name="handover",
    )(
        *[
            pltpu.with_memory_space_constraint(a, pltpu.HBM)
            for a in (
                prompt,
                gain_first.reshape(1, -1), gate_first, up_first, down_first,
                gain_second.reshape(1, -1), gate_second, up_second, down_second,
            )
        ],
    )
    outs = pl.pallas_call(
        hand_out,
        out_shape=shapes,
        in_specs=[pl.BlockSpec(memory_space=vmem)] * 7,
        out_specs=(pl.BlockSpec(memory_space=pl.ANY),) * 7,
        scratch_shapes=[sem((7,))],
        compiler_params=pltpu.CompilerParams(vmem_limit_bytes=16 * 1024 * 1024),
        name="hand_out",
    )(*outs)
    return (outs[0].T, outs[1].T, outs[2], outs[3].T, outs[4].T, outs[5], outs[6])


LIMIT = 44 * 1024 * 1024


def solution(mesh):
    rows = P(("gr", "fs"), None)
    block = P(("gr", "fs"), "tp")
    line = P(("gr", "fs"))
    return jax.shard_map(
        shards,
        mesh=mesh,
        in_specs=(rows, line, block, block, block, line, block, block, block),
        out_specs=(
            P(None, "tp"),
            P(None, "tp"),
            P("tp", None),
            P(None, "tp"),
            P(None, "tp"),
            P("tp", None),
            P(("gr", "fs", "tp"), None),
        ),
        check_vma=False,
    )
```

```python
import functools
import heapq

import jax
import jax.numpy as jnp
from jax import lax
from jax.experimental import pallas as pl
from jax.experimental.pallas import tpu as pltpu
from jax.sharding import PartitionSpec as P

MESH = pl.DeviceIdType.MESH
F32, BF16 = jnp.float32, jnp.bfloat16
NX, NY, NZ = 4, 4, 8
CHUNKS = 4
WAVES = 2
WAVE = 64 // WAVES
GROUPS = ((2,), (1, 3), (0,))

UNIT, SQUARE, DOWN, ROWS, PAIR, WIRE, NEAR = 1.15, 1.05, 2.1, 5.7, 0.5, 2.1, 1.0

ZP, ZM, XP, XM, YP, YM, PR = LINKS = range(7)
STEP = {ZP: (1, 0, 0), ZM: (-1, 0, 0), XP: (0, 1, 0), XM: (0, -1, 0), YP: (0, 0, 1), YM: (0, 0, -1), PR: (0, 0, 0)}
G, U, D, N, R, E = range(6)
BEGIN, START, NORM, HIDE, GLUE, TURN, PART, SUM, LAST, SOURCE, PASS = range(100, 111)
OWN, ALONG, ACROSS, PAIRED, FAR, CLOSE, GIVE = range(200, 207)


class Copy:
    def __init__(self, idx, link, dur, at):
        self.idx, self.link, self.dur = idx, link, dur
        self.buf = at["buf"]
        self.at = at
        self.rank = 0


class Task:
    def __init__(self, needs, dur, sends, rank, only):
        self.needs, self.dur, self.sends, self.rank, self.only = list(needs), dur, list(sends), rank, only

    def falls_to(self, d):
        return self.only is None or min(d, NZ - d) == self.only


class Plan:
    def __init__(self):
        self.copies, self.tasks = {}, {}

    def copy(self, key, link, dur, **at):
        self.copies[key] = Copy(len(self.copies), link, dur, at)
        return key

    def task(self, key, needs, dur, sends=(), rank=0, only=None):
        self.tasks[key] = Task(needs, dur, sends, rank, only)

    def starts_here(self, c, d):
        if c.buf != D or c.at["kind"] == ACROSS:
            return True
        if c.at["kind"] == OWN:
            return d != 0
        return d < 4 if c.link == ZP else d == 0 or d > 5

    def absent(self, need, d):
        if need in self.tasks:
            return not self.tasks[need].falls_to(d)
        copy = self.copies.get(need)
        if copy is None or copy.buf != D:
            return False
        if copy.at["kind"] == OWN:
            return d != 0
        return copy.at["kind"] == ALONG and (d == 0 or (copy.link == ZP) != (d < 5))

    def simulate(self, fixed=None):
        kinds = [(d, c) for d in range(NZ) for c in range(2)]
        left = {k: {t: {n for n in v.needs if not self.absent(n, k[0])} for t, v in self.tasks.items() if v.falls_to(k[0])} for k in kinds}
        users = {}
        for t, v in self.tasks.items():
            for n in v.needs:
                users.setdefault(n, []).append(t)
        place = {t: i for i, t in enumerate(self.tasks)}
        ready, pending, turn = {k: [] for k in kinds}, {}, {k: 0 for k in kinds}
        free, busy = {}, {k: 0.0 for k in kinds}
        starts = {k: {} for k in kinds}
        events, self.count = [], 0

        def at_time(at, k, link, what):
            self.count += 1
            heapq.heappush(events, (at, self.count, k, link, what))

        def enable(k, t, at):
            rank = self.tasks[t].rank
            heapq.heappush(ready[k], (rank, place[t] if rank else at, place[t], t))

        def start(k, key, only, now):
            copy = self.copies[key]
            d, c = k
            starts[k][key, only] = now
            end = free[k, copy.link] = max(now, free.get((k, copy.link), 0.0)) + copy.dur
            dz, _, dy = STEP[copy.link]
            to = ((d + dz - 2 * dy) % NZ, c)
            if copy.buf == D and copy.at["kind"] == OWN:
                to = (0, c)
            if copy.link == PR:
                to = ((d + (-1 if c == 0 else 1)) % NZ, 1 - c)
            at_time(end + (NEAR if copy.link == PR else WIRE), to, None, key)

        for k in kinds:
            for t in left[k]:
                if not left[k][t]:
                    enable(k, t, 0.0)
            at_time(0.0, k, None, None)
        while events:
            now, _, k, link, what = heapq.heappop(events)
            if link is not None:
                queue = pending[k, link]
                if queue and now >= free.get((k, link), 0.0) - ahead(queue[0][0]) - 1e-9:
                    _, _, key, only = heapq.heappop(queue)
                    start(k, key, only, now)
                if queue:
                    at_time(max(now, free.get((k, link), 0.0) - ahead(queue[0][0])), k, link, None)
                continue
            for t in users.get(what, ()) if what is not None else ():
                if what in left[k].get(t, ()):
                    left[k][t].discard(what)
                    if not left[k][t]:
                        enable(k, t, now)
            if what in self.tasks and fixed is None:
                task = self.tasks[what]
                for key in task.sends:
                    copy = self.copies[key]
                    if self.starts_here(copy, k[0]):
                        self.count += 1
                        heapq.heappush(pending.setdefault((k, copy.link), []), (copy.rank, self.count, key, task.only))
                        at_time(max(now, free.get((k, copy.link), 0.0) - ahead(copy.rank)), k, copy.link, None)
            if now < busy[k]:
                continue
            if fixed is None:
                if not ready[k]:
                    continue
                t = heapq.heappop(ready[k])[3]
            else:
                t = None
                while turn[k] < len(fixed):
                    key, only = fixed[turn[k]]
                    if key in self.tasks:
                        if key in left[k]:
                            if not left[k][key]:
                                t = key
                                turn[k] += 1
                            break
                    elif (only is None or min(k[0], NZ - k[0]) == only) and self.starts_here(self.copies[key], k[0]):
                        start(k, key, only, now)
                    turn[k] += 1
                if t is None:
                    continue
            starts[k][t, None] = now
            busy[k] = now + self.tasks[t].dur
            at_time(busy[k], k, None, t)
        if fixed is not None and any(turn[k] < len(fixed) for k in kinds):
            return starts, 1e9
        return starts, max(busy.values())

    def find_before(self):
        starters, self.before = {}, {}
        for t, v in self.tasks.items():
            for c in v.sends:
                starters.setdefault(c, []).append((c, v.only))
                self.before[c, v.only] = [(t, None)]
        for t, v in self.tasks.items():
            before = [(n, None) for n in v.needs if n in self.tasks]
            for n in v.needs:
                for c, m in starters.get(n, ()):
                    hop = self.copies[n].buf == D and self.copies[n].at["kind"] == ALONG
                    if m is None or v.only is None or m == v.only - hop:
                        before.append((c, m))
            self.before[t, None] = before

    def line_up(self, starts, mix):
        at = {}
        for e in self.before:
            here = [v[e] for v in starts.values() if e in v]
            at[e] = mix * max(here) + (1 - mix) * sum(here) / len(here) if here else 0.0
        place = {e: i for i, e in enumerate(self.before)}
        changed = True
        while changed:
            changed = False
            for e, before in self.before.items():
                for n in before:
                    if at[n] >= at[e]:
                        at[e] = at[n] + 1e-6
                        changed = True
        return sorted(self.before, key=lambda e: (at[e], place[e]))

    def order(self):
        self.find_before()
        starts, self.ideal = self.simulate()
        best = None
        for mix in (0.0, 0.2, 0.4, 0.6, 0.8, 1.0):
            line = self.line_up(starts, mix)
            total = self.simulate(line)[1]
            if best is None or total < best[0]:
                best = total, line
        self.total = best[0]
        return best[1]


GIVEN = 4.5
GATE = (PASS, E, 0, ALONG, 0, 1)
RELAY = [(E, 0, GIVE, 4, 2)] * 2
AHEAD = 1.0
RANKS = [0, 0, -3, 23, 1, 3, 18, 20, 29, 34, 31, 37, 30, -50]


def ahead(rank):
    return AHEAD if rank >= 0 else 9.0


def rank_copies(p):
    for key, c in p.copies.items():
        if c.buf not in (G, U, D, E):
            continue
        l = c.at["layer"]
        if c.link in (YP, YM):
            r = 0
        elif c.link in (ZP, ZM):
            if c.buf == D:
                r = RANKS[0]
            elif c.buf in (G, E):
                r = RANKS[1] + RANKS[2] * key[-1]
            else:
                r = RANKS[3] + RANKS[4] * key[-1]
        elif c.buf == U:
            r = RANKS[5] if len(key) == 4 else RANKS[6]
        elif c.buf in (G, E):
            far = c.at["x"] == 2
            r = RANKS[9] if far else RANKS[7] if key[2] == OWN else RANKS[8]
        else:
            r = RANKS[11] if c.at["x"] == 2 else RANKS[10]
        c.rank = r + RANKS[12] * l + RANKS[13] * (c.buf == E)


def build_plan():
    p = Plan()
    whole, downs, blocks = ([], []), ([], []), {}
    signs = ((0, -1), (1, 1))
    zs, xs = (ZP, ZM), (XP, XM)

    p.task((BEGIN,), [], 3.0, [p.copy((D, 1, OWN), YP, 2.0, buf=D, layer=1, kind=OWN)])
    for l in (0, 1):

        def put(buf, link, zrel, xrel, half, *tag):
            key = (buf, l, *tag)
            unit = SQUARE if buf == E else UNIT
            p.copy(key, link, unit * (1.0 if half is None else 0.5), buf=buf, layer=l, z=zrel, x=xrel, half=half)
            (blocks.setdefault((zrel % NZ, xrel % NX), []) if buf == E else whole[l]).append(key)
            return key

        z_first = (G, E) if l == 0 else (G,)
        first = []
        for s, sign in signs:
            first += [put(b, zs[s], sign, 0, None, ALONG, s, 1) for b in z_first]
            first += [put(U, xs[s], 0, sign, None, ACROSS, s)]
            first += [put(U, zs[s], sign, 0, None, ALONG, 0, s, 1)]
            first += [put(b, xs[s], 0, sign, None, OWN, s) for b in z_first]
        p.task((START, l), [(BEGIN,)] if l == 0 else [(START, 0)], 0.2, first)

        for b in z_first:
            for s, sign in signs:
                p.task((PASS, b, l, OWN, s), [(b, l, OWN, s)], 0.03, [put(b, xs[s], 0, 2, s, OWN, s, 2)])
                for step in (1, 2, 3, 4):
                    zrel, half = sign * step, s if step == 4 else None
                    sends = []
                    if step < 4:
                        sends.append(put(b, zs[s], sign * (step + 1), 0, s if step == 3 else None, ALONG, s, step + 1))
                    for t, to in signs:
                        sends.append(put(b, xs[t], zrel, to, half, ACROSS, s, step, t))
                    p.task((PASS, b, l, ALONG, s, step), [(b, l, ALONG, s, step)], 0.03, sends)
                    far = put(b, xs[s], zrel, 2, half, ACROSS, s, step, 2)
                    p.task((PASS, b, l, ACROSS, s, step), [(b, l, ACROSS, s, step, s)], 0.03, [far])
        for s, sign in signs:
            p.task((PASS, U, l, ACROSS, s), [(U, l, ACROSS, s)], 0.03, [put(U, xs[s], 0, 2, s, ACROSS, s, 2)])
            sends = [put(U, zs[t], to, sign, None, ALONG, 1 + s, t, 1) for t, to in signs]
            p.task((PASS, U, l, ALONG, 1 + s), [(U, l, ACROSS, s)], 0.03, sends)
        sends = [put(U, zs[t], to, 2, None, ALONG, 3, t, 1) for t, to in signs]
        p.task((PASS, U, l, ALONG, 3), [(U, l, ACROSS, 0, 2), (U, l, ACROSS, 1, 2)], 0.03, sends)
        for column, xrel in enumerate((0, -1, 1, 2)):
            for t, sign in signs:
                for step in range(1, 4 if (t == 0) == (column in (0, 2)) else 3):
                    c = put(U, zs[t], sign * (step + 1), xrel, None, ALONG, column, t, step + 1)
                    p.task((PASS, U, l, ALONG, column, t, step), [(U, l, ALONG, column, t, step)], 0.03, [c])

    for k in range(NZ):
        for j in range(NX):
            c = p.copy((E, 0, GIVE, k, j), (YP, YM)[k % 2], GIVEN / NX, buf=E, layer=0, k=k, x=j)
            p.task((PASS, E, 0, GIVE, k, j), blocks.get((k, j), []) + [(START, 0)], 0.04, [c])
            downs[0].extend([c, (PASS, E, 0, GIVE, k, j)])
    for cc in (0, 1):
        c = p.copy((E, 0, FAR, cc), (YP, YM)[cc], GIVEN, buf=E, layer=0, far=cc)
        p.task((PASS, E, 0, FAR, cc), [(PASS, E, 0, GIVE, k, j) for k in range(NZ) for j in range(NX)] + [RELAY[cc]], 0.05, [c])
        downs[0].append((PASS, E, 0, FAR, cc))
    l, along = 1, {}
    for k in range(CHUNKS):
        for s, sign in signs:
            along[k, s] = p.copy((D, l, ALONG, k, s), zs[s], DOWN, buf=D, layer=l, kind=ALONG, chunk=k)
        sends = [along[k, 0], along[k, 1]]
        sends += [p.copy((D, l, ACROSS, k, s), xs[s], DOWN, buf=D, layer=l, kind=ACROSS, chunk=k, x=sign) for s, sign in signs]
        s = k % 2
        c = p.copy((D, l, ACROSS, k, 2), xs[s], DOWN, buf=D, layer=l, kind=ACROSS, chunk=k, x=2)
        for m in range(NZ // 2 + 1):
            needs = [(SOURCE, l)] if m == 0 else [along[k, 0], along[k, 1]]
            p.task((PASS, D, l, ALONG, k, m), needs, 0.05, sends, only=m)
            p.task((PASS, D, l, ACROSS, k, m), [(D, l, ACROSS, k, s)], 0.03, [c], only=m)
            downs[l].append((PASS, D, l, ALONG, k, m))
        downs[l].extend([sends[2], sends[3], c])
    p.task((SOURCE, l), [(D, l, OWN), GATE], 0.1, [], only=0)

    p.task((NORM,), [(START, 0)], 2.0, rank=1)
    p.task((HIDE, 0), [(NORM,)] + whole[0], 3.0, rank=1)
    p.task((GLUE, 0), downs[0], 0.8, rank=1)
    add_reduce(p, 0, [(HIDE, 0), (GLUE, 0)])
    for w in range(WAVES):
        for s, sign in signs:
            c = p.copy((N, w, CLOSE, s), (YP, YM)[s], ROWS / WAVES, buf=N, wave=w, y=sign, half=None, core=0)
            p.tasks[LAST, 0, w].sends.append(c)
            far = p.copy((N, w, FAR, s), (YP, YM)[s], ROWS / WAVES / 2, buf=N, wave=w, y=2, half=s, core=0)
            near = p.copy((N, w, PAIRED, s), PR, PAIR / WAVES, buf=N, wave=w, y=sign, half=None, core=1)
            p.task((PASS, N, w, CLOSE, s), [c], 0.03, [far, near])
            c = p.copy((N, w, PAIRED, FAR, s), PR, PAIR / WAVES / 2, buf=N, wave=w, y=2, half=s, core=1)
            p.task((PASS, N, w, FAR, s), [far], 0.03, [c])
        p.tasks[LAST, 0, w].sends.append(p.copy((N, w, PAIRED), PR, PAIR / WAVES, buf=N, wave=w, y=0, half=None, core=1))
        rows = {
            (0,): [(LAST, 0, w), (N, w, PAIRED)],
            (1, 3): [(N, w, CLOSE, 0), (N, w, PAIRED, 0), (N, w, CLOSE, 1), (N, w, PAIRED, 1)],
            (2,): [(N, w, FAR, 0), (N, w, FAR, 1), (N, w, PAIRED, FAR, 0), (N, w, PAIRED, FAR, 1)],
        }
        for rs in GROUPS[::-1]:
            p.task((HIDE, 1, w, rs), rows[rs] + whole[1], 1.2, rank=1)
    p.task((GLUE, 1), downs[1], 0.8, rank=1)
    add_reduce(p, 1, [(GLUE, 1)])
    for l in (0, 1):
        for buf in (G, U):
            for part in (0, 1):
                p.task((TURN, buf, l, part), whole[l] + [(HIDE, 0)], 0.5, rank=2)
    rank_copies(p)
    p.sequence = p.order()
    return p


def add_reduce(p, l, needs):
    for w in range(WAVES):
        for rs in GROUPS:
            c = [p.copy((R, l, w, PAIRED, r), PR, PAIR / WAVES, buf=R, layer=l, wave=w, kind=PAIRED, rel=r) for r in rs]
            p.task((PART, l, w, rs), needs + ([(HIDE, 1, w, rs)] if l else []), 0.7, c, rank=1)
        far, near = [
            [p.copy((R, l, w, kind, s), (YP, YM)[s], ROWS / WAVES / part, buf=R, layer=l, wave=w, kind=kind, side=s) for s in (0, 1)]
            for kind, part in ((FAR, 2), (CLOSE, 1))
        ]
        p.task((SUM, l, w, 2), [(PART, l, w, (2,)), (R, l, w, PAIRED, 2)], 0.15, far)
        for s, r in enumerate((1, 3)):
            p.task((SUM, l, w, r), [(PART, l, w, (1, 3)), (R, l, w, PAIRED, r), far[s]], 0.15, [near[s]])
        p.task((LAST, l, w), [(PART, l, w, (0,)), (R, l, w, PAIRED, 0)] + near, 0.4)


def normalized(rows):
    scale = lax.rsqrt(jnp.mean(rows * rows, axis=-1, keepdims=True) + 1e-06)
    return (rows * scale).astype(BF16)


def gated(normed, w_gate, w_up):
    gate = jnp.dot(normed, w_gate, preferred_element_type=F32)
    upper = jnp.dot(normed, w_up, preferred_element_type=F32)
    return (gate / (1.0 + jnp.exp(-gate)) * upper).astype(BF16)


def kernel(
    plan,
    prompt_hbm,
    gain_a, gate_a, up_a, down_a,
    gain_b, gate_b, up_b, down_b,
    gt0, ut0, t0, gt1, ut1, t1, mixed,
    prompt, normed, hidden, part, stream,
    g0, u0, g1, u1, squares, given, relayed, d1, stage,
    pair0, pair1, far0, far1, near0, near1, sums,
    gains, gates, depths,
    load_sem, send_sem, recv_sem, own_sem,
):
    gr, fs, tp = lax.axis_index("gr"), lax.axis_index("fs"), lax.axis_index("tp")
    z = gr * 4 + fs // 4
    x = lax.rem(fs, 4)
    y = tp // 2
    core = lax.rem(tp, 2)

    def device(xx, yy, zz, cc):
        return (zz // 4, lax.rem(zz, 4) * 4 + xx, yy * 2 + cc)

    def zat(k):
        return lax.rem(z + (k % NZ), NZ) if k % NZ else z

    def xat(k):
        return lax.rem(x + (k % NX), NX) if k % NX else x

    def yat(k):
        return lax.rem(y + (k % NY), NY) if k % NY else y

    other = 1 - core
    peers = {
        ZP: device(x, y, zat(1), core),
        ZM: device(x, y, zat(-1), core),
        XP: device(xat(1), y, z, core),
        XM: device(xat(-1), y, z, core),
        YP: device(x, yat(1), z, core),
        YM: device(x, yat(-1), z, core),
        PR: device(x, y, z, other),
    }
    weights = {(G, 0): g0, (U, 0): u0, (G, 1): g1, (U, 1): u1}
    turned = {(G, 0): gt0, (U, 0): ut0, (G, 1): gt1, (U, 1): ut1}
    talls = (t0, t1)
    pairs, fars, nears = (pair0, pair1), (far0, far1), (near0, near1)
    dist = lax.rem(z + NZ - tp, NZ)

    def rows_at(ref, row, half):
        if half is None:
            return ref.at[pl.ds(pl.multiple_of(row, 64), 64), :]
        return ref.at[pl.ds(pl.multiple_of(row + 32 * half, 32), 32), :]

    def refs(c, sender):
        dz, dx, dy = STEP[c.link] if sender else (0, 0, 0)
        at = c.at
        if c.buf == E:
            ref = squares.at[zat(at["z"] + dz) * NX + xat(at["x"] + dx)]
            if at["half"] is not None:
                ref = ref.at[:, pl.ds(128 * at["half"], 128)]
            return ref, ref
        if c.buf in (G, U):
            row = (zat(at["z"] + dz) * NX + xat(at["x"] + dx)) * 64
            ref = rows_at(weights[c.buf, at["layer"]], row, at["half"])
            return ref, ref
        if c.buf == D:
            n = 8 // CHUNKS
            ref = d1.at[xat(at.get("x", 0) + dx), pl.ds(at["chunk"] * n, n)]
            return ref, ref
        w = at["wave"]
        if c.buf == N:
            cc = other if at["core"] and not sender else core
            row, size = (yat(at["y"] + dy) * 2 + cc) * 64 + WAVE * w, WAVE
            if at["half"] is not None:
                row, size = row + WAVE // 2 * at["half"], WAVE // 2
            ref = normed.at[pl.ds(pl.multiple_of(row, WAVE // 2), size), :]
            return ref, ref
        l, wave = at["layer"], pl.ds(WAVE * w, WAVE)
        if at["kind"] == PAIRED:
            row = (yat(at["rel"]) * 2 + other) * 64 + WAVE * w
            return part.at[l, pl.ds(pl.multiple_of(row, WAVE), WAVE), :], pairs[l].at[at["rel"], wave, :]
        side = at["side"]
        if at["kind"] == FAR:
            half = WAVE // 2
            return sums.at[l, 2, pl.ds(WAVE * w + half * side, half), :], fars[l].at[side, pl.ds(half * w, half), :]
        return sums.at[l, 1 + 2 * side, wave, :], nears[l].at[side, wave, :]

    def describe(c, sender):
        src, dst = refs(c, sender)
        return pltpu.make_async_remote_copy(
            src_ref=src,
            dst_ref=dst,
            send_sem=send_sem.at[c.idx],
            recv_sem=recv_sem.at[c.idx],
            device_id=peers[c.link],
            device_id_type=MESH,
        )

    def own_copy(c, t):
        return pltpu.make_async_remote_copy(
            src_ref=stage,
            dst_ref=d1.at[x, t],
            send_sem=send_sem.at[c.idx],
            recv_sem=own_sem.at[1, t],
            device_id=device(x, z // 2, z, lax.rem(z, 2)),
            device_id_type=MESH,
        )

    def passing(ref, sem):
        return pltpu.make_async_remote_copy(
            src_ref=ref, dst_ref=ref, send_sem=send_sem.at[0], recv_sem=sem, device_id=peers[PR], device_id_type=MESH
        )

    onward, back = [lax.rem(y + 1 + 2 * cc, NY) for cc in (core, other)]

    def given_copy(c, t, way=False):
        to = zat(c.at["k"])
        return pltpu.make_async_remote_copy(
            src_ref=squares.at[to * NX + xat(c.at["x"])],
            dst_ref=relayed.at[lax.rem(to, 2), xat(c.at["x"])] if way else given.at[t, xat(c.at["x"])],
            send_sem=send_sem.at[c.idx],
            recv_sem=own_sem.at[2, lax.rem(to, 2)] if way else own_sem.at[0, t],
            device_id=(gr, fs, onward * 2 + core) if way else (gr, fs, to),
            device_id_type=MESH,
        )

    def far_copy(c):
        cc, t = c.at["far"], back * 2 + core
        return pltpu.make_async_remote_copy(
            src_ref=relayed.at[cc],
            dst_ref=given.at[t],
            send_sem=send_sem.at[c.idx],
            recv_sem=own_sem.at[0, t],
            device_id=(gr, fs, onward * 2 + cc),
            device_id_type=MESH,
        )

    def passes(c):
        if "k" in c.at:
            return zat(c.at["k"]) != tp
        if c.buf != D or c.at["kind"] == ACROSS:
            return None
        if c.at["kind"] == OWN:
            return dist != 0
        return dist < 4 if c.link == ZP else jnp.logical_or(dist == 0, dist > 5)

    def if_so(here, act):
        if here is None:
            act()
        else:
            pl.when(here)(act)

    def is_own(c):
        return c.buf == D and c.at["kind"] == OWN

    def outgoing(c):
        if "far" in c.at:
            return far_copy(c)
        return given_copy(c, tp) if "k" in c.at else own_copy(c, tp) if is_own(c) else describe(c, True)

    def send(c, here):
        if "k" in c.at:
            opposite = lax.rem(zat(c.at["k"]) // 2 + NY - y, NY) == 2
            if_so(opposite, given_copy(c, tp, True).start)
            here = jnp.logical_and(here, jnp.logical_not(opposite))
        if_so(here, outgoing(c).start)

    def sent(c):
        if_so(passes(c), outgoing(c).wait_send)

    seen = set()

    def arrived(key, only):
        c = plan.copies[key]
        if "k" in c.at:
            t = c.at["k"]
            if c.at["x"] == 0:
                whole = given.at[t]
                if_so(tp != t, passing(whole, own_sem.at[0, t]).wait_recv)
            return
        if c.buf == D and c.at["kind"] == ALONG:
            if_so(dist == (only if c.link == ZP else NZ - only), describe(c, False).wait_recv)
            return
        if (key, only) in seen or (only is None and (key, 4) in seen):
            return
        seen.add((key, only))
        if is_own(c):
            for t in range(8):
                if_so(jnp.logical_and(dist == 0, tp != t), own_copy(c, t).wait_recv)
            return
        here = None if only is None else hops == only
        if_so(here, describe(c, False).wait_recv)

    hops = jnp.minimum(dist, NZ - dist)
    eye = lax.broadcasted_iota(jnp.int32, (64, 64), 0) == lax.broadcasted_iota(jnp.int32, (64, 64), 1)

    def fold(gain, w):
        column = jnp.sum(jnp.where(eye, gain[...], 0.0), axis=1, keepdims=True)
        return (column * w[...]).astype(BF16)

    mine = pl.ds(pl.multiple_of((z * NX + x) * 64, 64), 64)

    def rows_of(r, cc, w):
        return pl.ds(pl.multiple_of((yat(r) * 2 + cc) * 64 + WAVE * w, WAVE), WAVE)

    def group(rs, w):
        return [rows_of(r, cc, w) for r in rs for cc in (0, 1)]

    loads = [
        pltpu.make_async_copy(src, dst, load_sem.at[i])
        for i, (src, dst) in enumerate(
            (
                (gain_a, gains.at[0]), (gate_a, gates.at[0]), (up_a, gates.at[1]), (down_a, depths.at[0]),
                (gain_b, gains.at[1]), (gate_b, gates.at[2]), (up_b, gates.at[3]), (down_b, depths.at[1]),
                (prompt_hbm, prompt),
            )
        )
    ]

    def begin():
        for load in loads:
            load.start()
        barrier = pltpu.get_barrier_semaphore()
        greet = [peers[k] for k in (ZP, ZM, XP, XM)]
        greet += [(gr, fs, lax.rem(tp + k, 8)) for k in range(1, 8)]
        for who in greet:
            pl.semaphore_signal(barrier, inc=1, device_id=who, device_id_type=MESH)
        for load in loads[:8]:
            load.wait()
        for i, ref in enumerate((g0, u0, g1, u1)):
            ref[mine, :] = fold(gains.at[i // 2], gates.at[i])
        squares[z * NX + x] = depths[0].astype(BF16)
        stage[...] = depths[1].astype(BF16)

        @pl.when(dist == 0)
        def _():
            d1[x, tp] = depths[1].astype(BF16)

        pl.semaphore_wait(barrier, len(greet))

    def norm():
        loads[8].wait()

        @pl.loop(0, 8)
        def _(i):
            at = pl.ds(pl.multiple_of(i * 64, 64), 64)
            normed[at, :] = normalized(prompt[at, :].astype(F32))

    def hide(l, w=None, rs=None):
        if l == 0:

            @pl.loop(0, 2)
            def _(i):
                at = pl.ds(pl.multiple_of(i * 256, 256), 256)
                hidden[at, :] = gated(normed[at, :], g0[...], u0[...])

            return
        spots = group(rs, w)
        out = gated(jnp.concatenate([normed[at, :] for at in spots], axis=0), g1[...], u1[...])
        for i, at in enumerate(spots):
            hidden[at, :] = out[WAVE * i : WAVE * (i + 1)]

    def turn(buf, l, piece):
        src, dst = weights[buf, l], turned[buf, l]

        @pl.loop(0, 4)
        def _(i):
            at = pl.ds(pl.multiple_of((piece * 4 + i) * 256, 256), 256)
            dst[:, at] = src[at, :].astype(F32).T.astype(BF16)

    def glue(l):
        if l == 0:
            for k in range(NX):
                given[tp, k] = squares[tp * NX + k]
        for t in range(8):
            blocks = [(given[t, k] if l == 0 else d1[k, t]).astype(F32) for k in range(NX)]
            rows = jnp.concatenate(blocks, axis=0)
            talls[l][:, 256 * t : 256 * (t + 1)] = rows.astype(BF16)

    def partial(l, w, rs):
        spots = group(rs, w)
        rows = jnp.concatenate([hidden[at, :] for at in spots], axis=0)
        out = jnp.dot(rows, talls[l][...], preferred_element_type=F32).astype(BF16)
        for i, at in enumerate(spots):
            part[l, at, :] = out[WAVE * i : WAVE * (i + 1)]

    def chip_sum(l, w, r):
        wave = slice(WAVE * w, WAVE * (w + 1))
        return part[l, rows_of(r, core, w), :].astype(F32) + pairs[l][r, wave, :].astype(F32)

    def add_up(l, w, r):
        total, half = chip_sum(l, w, r), WAVE // 2
        lower, upper = slice(WAVE * w, WAVE * w + half), slice(WAVE * w + half, WAVE * (w + 1))
        first, second = total[:half], total[half:]
        if r == 1:
            first = first + fars[l][0, half * w : half * (w + 1), :].astype(F32)
        if r == 3:
            second = second + fars[l][1, half * w : half * (w + 1), :].astype(F32)
        sums[l, r, lower, :] = first.astype(BF16)
        sums[l, r, upper, :] = second.astype(BF16)

    def last(l, w):
        wave = slice(WAVE * w, WAVE * (w + 1))
        total = chip_sum(l, w, 0) + nears[l][0, wave, :].astype(F32) + nears[l][1, wave, :].astype(F32)
        if l == 0:
            at = rows_of(0, core, w)
            rows = prompt[at, :].astype(F32) + 0.5 * total
            stream[wave, :] = rows
            normed[at, :] = normalized(rows)
        else:
            mixed[wave, :] = (stream[wave, :] + 0.5 * total).astype(BF16)

    work = {BEGIN: begin, NORM: norm, HIDE: hide, TURN: turn, GLUE: glue, PART: partial, SUM: add_up, LAST: last}
    for key, only in plan.sequence:
        if key in plan.copies:
            c = plan.copies[key]
            here = passes(c)
            if only is not None:
                here = hops == only if here is None else jnp.logical_and(here, hops == only)
            send(c, here)
            continue
        task = plan.tasks[key]
        for n in task.needs:
            if key[:2] == (PASS, E) and key[3] == FAR:
                continue
            if n in plan.copies and not (task.only == 4 and plan.copies[n].link == ZM and plan.copies[n].at.get("kind") == ALONG):
                arrived(n, task.only)
        if key[:2] == (PASS, E) and key[3] == FAR:
            passing(relayed.at[key[4]], own_sem.at[2, key[4]]).wait_recv()
        if key[0] in work:
            work[key[0]](*key[1:])
    for c in plan.copies.values():
        sent(c)


def hand_out(*refs):
    sources, targets, sem = refs[:7], refs[7:14], refs[14]
    copies = [pltpu.make_async_copy(a, b, sem.at[i]) for i, (a, b) in enumerate(zip(sources, targets))]
    for copy in copies:
        copy.start()
    for copy in copies:
        copy.wait()


def shards(prompt, gain_first, gate_first, up_first, down_first, gain_second, gate_second, up_second, down_second):
    plan = build_plan()
    rows, width = prompt.shape
    units = gate_first.shape[1]
    depth, columns = down_first.shape
    count = len(plan.copies)
    sem, vmem = pltpu.SemaphoreType.DMA, pltpu.VMEM
    block = rows // 8
    tall = jax.ShapeDtypeStruct((units, width), BF16)
    shapes = (tall,) * 6 + (jax.ShapeDtypeStruct((block, width), BF16),)
    outs = pl.pallas_call(
        functools.partial(kernel, plan),
        out_shape=shapes,
        in_specs=[pl.BlockSpec(memory_space=pltpu.HBM)] * 9,
        out_specs=(pl.BlockSpec(memory_space=vmem),) * 7,
        scratch_shapes=[
            vmem((rows, width), BF16),
            vmem((rows, width), BF16),
            vmem((rows, units), BF16),
            vmem((2, rows, width), BF16),
            vmem((block, width), F32),
            *[vmem((width, units), BF16)] * 4,
            vmem((NX * NZ, depth, columns), BF16),
            vmem((8, NX, depth, columns), BF16),
            vmem((2, NX, depth, columns), BF16),
            vmem((NX, 8, depth, columns), BF16),
            vmem((depth, columns), BF16),
            *[vmem((NY, block, width), BF16)] * 2,
            *[vmem((2, block // 2, width), BF16)] * 2,
            *[vmem((2, block, width), BF16)] * 2,
            vmem((2, NY, block, width), BF16),
            vmem((2, 1, gain_first.shape[0]), F32),
            vmem((4, *gate_first.shape), F32),
            vmem((2, depth, columns), F32),
            sem((9,)),
            sem((count,)),
            sem((count,)),
            sem((3, 8)),
        ],
        compiler_params=pltpu.CompilerParams(collective_id=0, has_side_effects=True, vmem_limit_bytes=LIMIT),
        name="handover",
    )(
        *[
            pltpu.with_memory_space_constraint(a, pltpu.HBM)
            for a in (
                prompt,
                gain_first.reshape(1, -1), gate_first, up_first, down_first,
                gain_second.reshape(1, -1), gate_second, up_second, down_second,
            )
        ],
    )
    outs = pl.pallas_call(
        hand_out,
        out_shape=shapes,
        in_specs=[pl.BlockSpec(memory_space=vmem)] * 7,
        out_specs=(pl.BlockSpec(memory_space=pl.ANY),) * 7,
        scratch_shapes=[sem((7,))],
        compiler_params=pltpu.CompilerParams(vmem_limit_bytes=16 * 1024 * 1024),
        name="hand_out",
    )(*outs)
    return (outs[0].T, outs[1].T, outs[2], outs[3].T, outs[4].T, outs[5], outs[6])


LIMIT = 44 * 1024 * 1024


def solution(mesh):
    rows = P(("gr", "fs"), None)
    block = P(("gr", "fs"), "tp")
    line = P(("gr", "fs"))
    return jax.shard_map(
        shards,
        mesh=mesh,
        in_specs=(rows, line, block, block, block, line, block, block, block),
        out_specs=(
            P(None, "tp"),
            P(None, "tp"),
            P("tp", None),
            P(None, "tp"),
            P(None, "tp"),
            P("tp", None),
            P(("gr", "fs", "tp"), None),
        ),
        check_vma=False,
    )
```
